32 devices in a mesh: ep: 8 (over z, x), tp: 4 (over y, core).
Axes of the slice: x: 2, y: 2, z: 4, core: 2. Of those that a mesh axis runs over, the one named last changes fastest.
Arguments:
- queries: bfloat16 [1024, 512], P('ep'), may hold values from -6 to 6
- key_vectors: bfloat16 [1024, 512], P('ep'), may hold values from -6 to 6
- values: bfloat16 [1024, 1024], P('ep', 'tp'), may hold values from -6 to 6
- out_gate: bfloat16 [1024, 1024], P('ep', 'tp'), may hold values from -6 to 6
- input_gate: float32 [1024, 2], P('ep'), may hold values from -8 to 130
- forget_gate: float32 [1024, 2], P('ep'), may hold values from -2 to 16
- mix_weight: bfloat16 [1024, 2048], P('tp'), may hold values from -0.1875 to 0.1875
- expert_input: bfloat16 [2048, 2048], P('ep'), may hold values from -6 to 6
- norm_gain: float32 [2048], replicated, may hold values from 0.1 to 1.9
- route_ids: int32 [2048, 4], P('ep'), may hold values from 0 to 7, all different within a row; in each aligned block of 256 rows (0 to 255, 256 to 511, ...) at most 256 rows name the same one
- route_weights: float32 [2048, 4], P('ep'), may hold values from 0.2 to 1.2
- expert_gate: bfloat16 [32, 2048, 256], P(('ep', 'tp')), may hold values from -0.125 to 0.125
- expert_up: bfloat16 [32, 2048, 256], P(('ep', 'tp')), may hold values from -0.125 to 0.125
- expert_down: bfloat16 [32, 256, 2048], P(('ep', 'tp')), may hold values from -0.1875 to 0.1875
- shared_gate: bfloat16 [2048, 512], P(None, 'tp'), may hold values from -0.125 to 0.125
- shared_up: bfloat16 [2048, 512], P(None, 'tp'), may hold values from -0.125 to 0.125
- shared_down: bfloat16 [512, 2048], P('tp'), may hold values from -0.25 to 0.25
Outputs:
- mixer_out: bfloat16 [1024, 2048], P('ep')
- expert_out: bfloat16 [2048, 2048], P('ep')
The draws below stay inside these ranges and needn't reach their ends.
Inputs may be any that keep to these rules, and one draw needn't show every extreme that they name: `route_ids`: each row names 4 different experts. In each aligned block of 256 rows (the rows of one index of ep) no expert is named by more than 256 rows, and in some block one expert is named by exactly 256 rows.
All inputs are finite; a program needn't handle non-finite values.
Results may differ from the reference program's by a relative error of at most 0.01575.
Values may be sent and summed in bfloat16 or wider, within the bound.
A program may use at most 64 MiB of HBM per device.

```python
import math
import jax
import jax.numpy as jnp
import numpy as np
from jax import lax

D = 2048
MEMORY_HEADS = 2
KEY_DIM = 256
VAL_DIM = 512
BLOCK = 128
MOE_DEV = 256
TOPK = 4
FF = 1024
FF_SHARED = 512
MIXER_TOKEN_COUNT = 1024
MOE_TOKENS = 2048
TP_GROUP = 4
FF_DEV = 256
EXPERTS = 8
CAP = 256
VAL_DEV = 256
N_EP = 8
N_TP = 4


def draw_input_gate(key, part):
    random_subkeys = jax.random.split(jax.random.fold_in(key, 23), 1)
    pre_gate = jnp.clip(1.5 * jax.random.normal(random_subkeys[0], (MIXER_TOKEN_COUNT, MEMORY_HEADS), jnp.float32), -7.5, 7.5)
    return pre_gate


def draw_forget_gate(key, part):
    random_subkeys = jax.random.split(jax.random.fold_in(key, 41), 5)
    token_positions = jnp.arange(MIXER_TOKEN_COUNT, dtype=jnp.int32)
    shuffled = jax.random.permutation(random_subkeys[0], MEMORY_HEADS)
    slow_heads = (shuffled < MEMORY_HEADS // 2).astype(jnp.float32)
    slow_rate = 0.5
    baseline_rate = slow_heads * (slow_rate / MIXER_TOKEN_COUNT) + (1.0 - slow_heads) / 40.0
    block_multiplier = jnp.exp(jax.random.uniform(random_subkeys[1], (MIXER_TOKEN_COUNT // BLOCK, MEMORY_HEADS), jnp.float32, -0.69, 0.69))
    block_multiplier = jnp.repeat(block_multiplier, BLOCK, axis=0)
    jitter_amount = jnp.exp(jax.random.uniform(random_subkeys[2], (MIXER_TOKEN_COUNT, MEMORY_HEADS), jnp.float32, -1.1, 1.1))
    spike_position = jax.random.randint(random_subkeys[3], (3, MEMORY_HEADS), 0, MIXER_TOKEN_COUNT)
    spike_flag = jnp.any(token_positions[:, None, None] == spike_position[None, :, :], axis=1)
    spike_magnitude = jnp.log(jax.random.uniform(random_subkeys[4], (MIXER_TOKEN_COUNT, MEMORY_HEADS), jnp.float32, 0.5, 0.8))
    log_retention = -baseline_rate[None, :] * block_multiplier * jitter_amount + jnp.where(spike_flag, spike_magnitude, 0.0)
    return log_retention - jnp.log(-jnp.expm1(log_retention))


def levels(stream_key, dims, shards, least, high):
    def one(dim, shards_of):
        steps = jax.random.uniform(jax.random.fold_in(jax.random.fold_in(stream_key, 6), dim), (shards_of,), jnp.float32, least / len(shards), high / len(shards))
        return jnp.repeat(jnp.exp(steps), dims[dim] // shards_of).reshape((-1,) + (1,) * (len(dims) - dim - 1))

    factor_of = one(*shards[0])
    for cut in shards[1:]:
        factor_of = factor_of * one(*cut)
    return factor_of


def deal_out(stream_key, own, number, rows, count, top, limit, lean):
    order = jax.random.permutation(stream_key, count)
    crowded, ordinary = shares(count, rows * top, limit, lean, True), shares(count, rows * top, limit, lean, False)
    places = jnp.arange(count)

    def named(tallies, rotation):
        used = int((tallies > 0).sum())
        fixed = max(1, used // 4)
        shifted = fixed + (places - fixed + rotation * (used - fixed)) % max(1, count - fixed)
        return jnp.zeros((count,), jnp.int32).at[order[jnp.where(places < fixed, places, shifted)]].set(jnp.asarray(tallies, jnp.int32))

    tallies = jnp.where(number % 4 == 0, named(crowded, number // 4), named(ordinary, number - number // 4 - 1))
    mixed = jax.random.permutation(jax.random.fold_in(own, 3), count)
    donor, sink = mixed[0:count // 2 * 2:2], mixed[1:count // 2 * 2:2]
    margin = jnp.minimum(tallies[donor] - 1, limit - tallies[sink]) // 2
    margin = jnp.where((donor == order[0]) | (sink == order[0]) | (tallies[sink] == 0), 0, jnp.maximum(margin, 0))
    shifted = jax.random.randint(jax.random.fold_in(own, 4), (count // 2,), 0, 1 << 20) % (margin + 1)
    tallies = tallies.at[donor].add(-shifted).at[sink].add(shifted)
    members = jnp.searchsorted(jnp.cumsum(tallies), jnp.arange(rows * top), side="right").astype(jnp.int32)
    grid = members.reshape(top, rows).T
    grid = grid[jax.random.permutation(jax.random.fold_in(own, 1), rows)]
    rotation = jax.random.randint(jax.random.fold_in(own, 2), (rows, 1), 0, top)
    return jnp.take_along_axis(grid, (jnp.arange(top)[None, :] + rotation) % top, axis=1)


def shares(count, total, limit, skew, full):
    weights = [(1 << 20) // math.isqrt(standing ** skew) + 1 for standing in range(1, count + 1)]
    largest = limit if full else min(limit, max(-(-total // count), total * weights[0] // sum(weights)))
    least = 1 if total - largest >= count - 1 else 0
    given, rest = [largest] + [least] * (count - 1), total - largest - least * (count - 1)
    while rest > 0:
        free = [i for i in range(1, count) if given[i] < largest] or [i for i in range(1, count) if given[i] < limit]
        pool, left = sum([weights[i] for i in free]), rest
        for i in free:
            extra = min(limit - given[i], max(1, left * weights[i] // pool), rest)
            given[i] = given[i] + extra
            rest = rest - extra
    return np.array(given)


def centred(rng, shape, width, reach, shards=(), held_as=jnp.bfloat16):
    entries = width * jax.random.normal(rng, shape, jnp.float32)
    if shards:
        entries = entries * levels(rng, shape, shards, -0.22, 0.18)
    return jnp.clip(entries, -reach, reach).astype(held_as)


def setup_inputs(seed: int = 0) -> dict:
    keys = jax.random.split(jax.random.key(seed), 18)
    queries = centred(keys[0], (MIXER_TOKEN_COUNT, MEMORY_HEADS * KEY_DIM), 1.0, 6.0, ((0, 8),))
    key_vectors = centred(keys[1], (MIXER_TOKEN_COUNT, MEMORY_HEADS * KEY_DIM), 1.0, 6.0, ((0, 8),))
    values = centred(keys[2], (MIXER_TOKEN_COUNT, MEMORY_HEADS * VAL_DIM), 1.0, 6.0, ((0, 8), (1, 4)))
    out_gate = centred(keys[3], (MIXER_TOKEN_COUNT, MEMORY_HEADS * VAL_DIM), 1.0, 6.0, ((0, 8), (1, 4)))
    input_gate = draw_input_gate(jax.random.fold_in(keys[17], 71), 0)
    forget_gate = draw_forget_gate(jax.random.fold_in(keys[17], 71), 0)
    mix_weight = centred(keys[6], (MEMORY_HEADS * VAL_DIM, D), (MEMORY_HEADS * VAL_DIM) ** -0.5, 0.1875, ((0, 4),))
    expert_input = centred(keys[7], (MOE_TOKENS, D), 1.0, 6.0, ((0, 8),))
    norm_gain = jnp.clip(1.0 + 0.18 * jax.random.normal(keys[8], (D,), jnp.float32), 0.1, 1.9)
    route_ids_keys = jax.random.split(jax.random.fold_in(keys[9], 1), MOE_TOKENS // MOE_DEV)
    route_ids_turns = jax.random.permutation(jax.random.fold_in(keys[9], 3), MOE_TOKENS // MOE_DEV)
    route_ids = jax.vmap(lambda own, number: deal_out(jax.random.fold_in(keys[9], 2), own, number, MOE_DEV, EXPERTS, TOPK, CAP, 2))(route_ids_keys, route_ids_turns).reshape((MOE_TOKENS, TOPK))
    route_weights = jnp.clip(0.2 + 1 * jax.random.uniform(keys[10], (MOE_TOKENS, TOPK), jnp.float32) ** levels(keys[10], (MOE_TOKENS, TOPK), ((0, 8),), -0.2, 0.2), 0.2, 1.2)
    expert_gate = centred(keys[11], (EXPERTS * TP_GROUP, D, FF_DEV), D ** -0.5, 0.125, ((0, 32),))
    expert_up = centred(keys[12], (EXPERTS * TP_GROUP, D, FF_DEV), D ** -0.5, 0.125, ((0, 32),))
    expert_down = centred(keys[13], (EXPERTS * TP_GROUP, FF_DEV, D), FF ** -0.5, 0.1875, ((0, 32),))
    shared_gate = centred(keys[14], (D, FF_SHARED), D ** -0.5, 0.125, ((1, 4),))
    shared_up = centred(keys[15], (D, FF_SHARED), D ** -0.5, 0.125, ((1, 4),))
    shared_down = centred(keys[16], (FF_SHARED, D), FF_SHARED ** -0.5, 0.25, ((0, 4),))
    return dict(queries=queries, key_vectors=key_vectors, values=values, out_gate=out_gate, input_gate=input_gate, forget_gate=forget_gate, mix_weight=mix_weight, expert_input=expert_input, norm_gain=norm_gain, route_ids=route_ids, route_weights=route_weights, expert_gate=expert_gate, expert_up=expert_up, expert_down=expert_down, shared_gate=shared_gate, shared_up=shared_up, shared_down=shared_down)


epsilon = 1e-06
den_floor = 4.0

def mixer_part(queries, key_vectors, values, out_gate, input_gate, forget_gate, mix_weight):
    length = queries.shape[0]
    blocks = length // BLOCK
    factor = KEY_DIM ** (-0.5)
    causal = jnp.tril(jnp.ones((BLOCK, BLOCK), dtype=bool))

    def by_head(matrix, columns):
        return matrix.reshape(blocks, BLOCK, MEMORY_HEADS, columns).transpose(0, 2, 1, 3)
    query_blocks = by_head(queries, KEY_DIM)
    key_blocks = by_head(key_vectors, KEY_DIM)
    value_blocks = by_head(values, VAL_DIM)
    input_blocks = input_gate.reshape(blocks, BLOCK, MEMORY_HEADS).transpose(0, 2, 1)
    forget_blocks = jax.nn.log_sigmoid(forget_gate).reshape(blocks, BLOCK, MEMORY_HEADS).transpose(0, 2, 1)

    def block_step(carry_in, inputs):
        memory, normalizer, running = carry_in
        query_block, key_block, value_block, input_block, forget_block = inputs
        cumulative = jnp.cumsum(forget_block, axis=-1)
        carried = cumulative + running[:, None]
        log_weight = cumulative[:, :, None] - cumulative[:, None, :] + input_block[:, None, :]
        log_weight = jnp.where(causal, log_weight, -jnp.inf)
        stabilizer = jnp.maximum(carried, lax.optimization_barrier(jnp.max(log_weight, axis=-1)))
        within = jnp.exp(log_weight - stabilizer[:, :, None])
        across = jnp.exp(carried - stabilizer)
        query_wide = query_block.astype(jnp.float32)
        key_wide = key_block.astype(jnp.float32)
        value_wide = value_block.astype(jnp.float32)
        scores = jnp.einsum('htd,hsd->hts', query_wide, key_wide) * factor
        weights = scores * within
        weights_low = lax.optimization_barrier(weights.astype(jnp.bfloat16)).astype(jnp.float32)
        scaled = query_wide * factor
        numerator = across[:, :, None] * jnp.einsum('htd,hdv->htv', scaled, memory, precision=lax.Precision.HIGHEST)
        numerator = numerator + jnp.einsum('hts,hsv->htv', weights_low, value_wide)
        denominator = across * jnp.einsum('htd,hd->ht', scaled, normalizer, precision=lax.Precision.HIGHEST)
        denominator = denominator + lax.optimization_barrier(jnp.sum(weights, axis=-1))
        hidden = numerator / jnp.maximum(jnp.abs(denominator), den_floor)[:, :, None]
        block_total = cumulative[:, -1]
        log_retention = block_total[:, None] - cumulative + input_block
        running_next = jnp.maximum(block_total + running, lax.optimization_barrier(jnp.max(log_retention, axis=-1)))
        carry_decay = jnp.exp(block_total + running - running_next)
        weighted_keys = key_wide * jnp.exp(log_retention - running_next[:, None])[:, :, None]
        memory = carry_decay[:, None, None] * memory + jnp.einsum('hsd,hsv->hdv', weighted_keys, value_wide, precision=lax.Precision.HIGHEST)
        normalizer = carry_decay[:, None] * normalizer + lax.optimization_barrier(jnp.sum(weighted_keys, axis=1))
        return ((memory, normalizer, running_next), hidden)
    initial = (jnp.zeros((MEMORY_HEADS, KEY_DIM, VAL_DIM), jnp.float32), jnp.zeros((MEMORY_HEADS, KEY_DIM), jnp.float32), jnp.zeros((MEMORY_HEADS,), jnp.float32))
    _, hidden = lax.scan(block_step, initial, (query_blocks, key_blocks, value_blocks, input_blocks, forget_blocks))
    hidden = hidden.transpose(0, 2, 1, 3).reshape(length, MEMORY_HEADS * VAL_DIM)
    gated_rows = (hidden * jax.nn.sigmoid(out_gate.astype(jnp.float32))).astype(jnp.bfloat16)

    def add_group(summed, group_index):
        offset = (group_index * VAL_DEV).astype(jnp.int32)
        partial_value = jnp.dot(lax.dynamic_slice_in_dim(gated_rows, offset, VAL_DEV, 1), lax.dynamic_slice_in_dim(mix_weight, offset, VAL_DEV, 0), preferred_element_type=jnp.float32)
        return (summed + lax.optimization_barrier(partial_value.astype(jnp.bfloat16)).astype(jnp.float32), None)
    summed, _ = lax.scan(add_group, jnp.zeros((length, D), jnp.float32), jnp.arange(N_TP, dtype=jnp.int32))
    return summed.astype(jnp.bfloat16)

def expert_part(expert_input, norm_gain, route_ids, route_weights, expert_gate, expert_up, expert_down, shared_gate, shared_up, shared_down):
    rows_wide = expert_input.astype(jnp.float32)
    normed = (rows_wide * lax.rsqrt(lax.optimization_barrier(jnp.mean(rows_wide * rows_wide, axis=-1, keepdims=True)) + epsilon) * norm_gain).astype(jnp.bfloat16)
    chosen = route_ids.reshape(N_EP, MOE_DEV * TOPK)
    onehot = (chosen[:, :, None] == jnp.arange(EXPERTS, dtype=jnp.int32)[None, None, :]).astype(jnp.int32)
    earlier = jnp.cumsum(onehot, axis=1) - onehot
    slot_rank = lax.optimization_barrier(jnp.sum(earlier * onehot, axis=2))
    slot_index = (jnp.arange(N_EP, dtype=jnp.int32)[:, None] * CAP + slot_rank).reshape(-1)
    expert_of = route_ids.reshape(-1)
    token_of = jnp.arange(MOE_TOKENS * TOPK, dtype=jnp.int32) // TOPK
    slot_token = jnp.zeros((EXPERTS, N_EP * CAP), jnp.int32).at[expert_of, slot_index].set(token_of)
    slot_weight = jnp.zeros((EXPERTS, N_EP * CAP), jnp.float32).at[expert_of, slot_index].set(route_weights.reshape(-1))

    def one_expert(routed, expert_index):
        tokens_here = slot_token[expert_index]
        weight_here = slot_weight[expert_index]
        picked = normed[tokens_here].astype(jnp.float32)
        rows_base = (expert_index * TP_GROUP).astype(jnp.int32)
        gate_w = lax.dynamic_slice_in_dim(expert_gate, rows_base, TP_GROUP, 0).astype(jnp.float32)
        up_w = lax.dynamic_slice_in_dim(expert_up, rows_base, TP_GROUP, 0).astype(jnp.float32)
        down_w = lax.dynamic_slice_in_dim(expert_down, rows_base, TP_GROUP, 0).astype(jnp.float32)
        gate_val = jnp.einsum('rd,gdf->rgf', picked, gate_w)
        up_val = jnp.einsum('rd,gdf->rgf', picked, up_w)
        hidden = lax.optimization_barrier((jax.nn.silu(gate_val) * up_val).astype(jnp.bfloat16)).astype(jnp.float32)
        partials = jnp.einsum('rgf,gfd->rgd', hidden, down_w)
        partials = lax.optimization_barrier(partials.astype(jnp.bfloat16)).astype(jnp.float32)
        result = lax.optimization_barrier(jnp.sum(partials, axis=1)) * weight_here[:, None]
        return (routed.at[tokens_here].add(result), None)
    routed, _ = lax.scan(one_expert, jnp.zeros((MOE_TOKENS, D), jnp.float32), jnp.arange(EXPERTS, dtype=jnp.int32))
    shared_gate_val = jnp.dot(normed, shared_gate, preferred_element_type=jnp.float32)
    shared_up_val = jnp.dot(normed, shared_up, preferred_element_type=jnp.float32)
    shared_act = (jax.nn.silu(shared_gate_val) * shared_up_val).astype(jnp.bfloat16)
    shared_rows = jnp.dot(shared_act, shared_down, preferred_element_type=jnp.float32)
    return (routed + shared_rows).astype(jnp.bfloat16)

def reference(queries, key_vectors, values, out_gate, input_gate, forget_gate, mix_weight, expert_input, norm_gain, route_ids, route_weights, expert_gate, expert_up, expert_down, shared_gate, shared_up, shared_down):
    mixer_out = mixer_part(queries, key_vectors, values, out_gate, input_gate, forget_gate, mix_weight)
    expert_out = expert_part(expert_input, norm_gain, route_ids, route_weights, expert_gate, expert_up, expert_down, shared_gate, shared_up, shared_down)
    return (mixer_out, expert_out)
```

```python
import functools

import jax
import jax.numpy as jnp
from jax import lax
from jax.experimental import pallas as pl
from jax.experimental.pallas import tpu as pltpu
from jax.sharding import PartitionSpec as P

D = 2048
MEMORY_HEADS = 2
KEY_DIM = 256
BLOCK = 128
FF = 1024


epsilon = 1e-06
lowest = -1e30
den_floor = 4.0


def mixer_local(queries, key_vectors, values, input_gate, forget_gate):
    tp_count = lax.axis_size("tp")
    tp_rank = lax.axis_index("tp")
    head_index = tp_rank // (tp_count // MEMORY_HEADS)
    offset = head_index * KEY_DIM
    query_head = lax.dynamic_slice_in_dim(queries, offset, KEY_DIM, 1)
    key_head = lax.dynamic_slice_in_dim(key_vectors, offset, KEY_DIM, 1)
    select = jnp.arange(MEMORY_HEADS, dtype=jnp.int32)[None, :] == head_index
    gates = jnp.stack(
        [
            jnp.sum(jnp.where(select, input_gate, 0.0), axis=1),
            jax.nn.log_sigmoid(jnp.sum(jnp.where(select, forget_gate, 0.0), axis=1)),
        ]
    )
    return query_head, jnp.concatenate([key_head, values], axis=1), gates


def mixer_rows(query_head, both, gates, out_gate):
    ep_count = lax.axis_size("ep")
    ep_rank = lax.axis_index("ep")
    length = query_head.shape[0]
    factor = KEY_DIM ** (-0.5)
    keys_all = both[:, :KEY_DIM]
    values_all = both[:, KEY_DIM:]
    total = ep_count * length
    blocks = total // BLOCK
    mine = length // BLOCK
    input_all = gates[0].reshape(blocks, BLOCK)
    cumulative = jnp.cumsum(gates[1].reshape(blocks, BLOCK), axis=1)
    block_total = cumulative[:, -1]
    index = jnp.arange(blocks, dtype=jnp.int32)
    here = ep_rank * mine + jnp.arange(mine, dtype=jnp.int32)
    between = (index[None, None, :] > index[None, :, None]) & (
        index[None, None, :] < here[:, None, None]
    )
    gap = jnp.sum(jnp.where(between, block_total[None, None, :], 0.0), axis=2)
    ahead = jnp.sum(jnp.where(index[None, :] < here[:, None], block_total[None, :], 0.0), axis=1)
    keep = block_total[:, None] - cumulative + input_all
    own_cumulative = lax.dynamic_slice_in_dim(cumulative, ep_rank * mine, mine, 0)
    same = index[None, :] == here[:, None]
    column = jnp.where(same[:, :, None], input_all - cumulative, keep + gap[:, :, None])
    log_weight = own_cumulative[:, :, None, None] + column[:, None]
    row_at = jnp.arange(BLOCK, dtype=jnp.int32)
    visible = (index[None, :] < here[:, None])[:, None, :, None] | (
        same[:, None, :, None] & (row_at[None, :, None, None] >= row_at[None, None, None, :])
    )
    log_weight = jnp.where(visible, log_weight, -jnp.inf).reshape(length, total)
    carried = (own_cumulative + ahead[:, None]).reshape(length)
    stabilizer = jnp.maximum(carried, jnp.max(log_weight, axis=1))
    within = jnp.exp(log_weight - stabilizer[:, None])
    scores = (
        jnp.einsum("td,sd->ts", query_head, keys_all, preferred_element_type=jnp.float32) * factor
    )
    weights = scores * within
    numerator = jnp.dot(
        weights.astype(jnp.bfloat16), values_all, preferred_element_type=jnp.float32
    )
    denominator = jnp.sum(weights, axis=1)
    hidden = numerator / jnp.maximum(jnp.abs(denominator), den_floor)[:, None]
    gated_rows = (hidden * jax.nn.sigmoid(out_gate.astype(jnp.float32))).astype(jnp.bfloat16)
    return gated_rows


splits = ((64, 16), (64, 16))
halves = 2


def lane_kernel(
    lines,
    ig_ref, fg_ref, gain_ref, ids_ref, rw_ref,
    q_ref, k_ref, v_ref, og_ref, mw_ref, x_ref, g_ref, u_ref, d_ref, sg_ref, su_ref, sd_ref,
    mo_ref, eo_ref,
    xbuf, qb, ogb, mwb, gall, uall, dall, sgall, suall, sdall, sall,
    tok, act, kvb, side, brow, stab, num, den, res, xin, zout, zin, mpart, mpeer, msum, mother,
    local, z_send, z_recv, x_send, x_recv, e_send, e_recv, kz_send, kz_recv, kx_send, kx_recv,
    s_send, s_recv, a_send, a_recv, b_send, b_recv, y_send, y_recv, f_send, f_recv,
    xo_send, xo_recv, zo_send, zo_recv, ey_send, ey_recv, eb_send, eb_recv, ef_send, ef_recv,
    m_send, m_recv,
):
    me = lax.axis_index("ep")
    j = lax.axis_index("tp")
    z, x = me // 2, me % 2
    y, c = j // 2, j % 2
    ep_count = 2 * lines
    rows = x_ref.shape[0] // 2
    length = q_ref.shape[0]
    key_dim = qb.shape[1]
    half = dall.shape[2]
    units = g_ref.shape[2]
    shared = sg_ref.shape[1]
    piece = half // halves
    part = length // 2
    low, wide = jnp.bfloat16, jnp.float32

    def remote(src, dst, send, recv, ep, tp):
        return pltpu.make_async_remote_copy(
            src_ref=src, dst_ref=dst, send_sem=send, recv_sem=recv,
            device_id={"ep": ep, "tp": tp}, device_id_type=pl.DeviceIdType.MESH,
        )

    across = z * 2 + 1 - x
    other_y = (1 - y) * 2 + c
    buddy = y * 2 + 1 - c

    def lanes(start, size):
        return pl.ds(pl.multiple_of(start, 128), size)

    def sublanes(start, size):
        return pl.ds(pl.multiple_of(start, 8), size)

    mine = lanes(y * half, half)
    theirs = lanes((1 - y) * half, half)
    heads = lanes(y * key_dim, key_dim)

    def load(n):
        pairs = (
            (x_ref.at[sublanes(c * rows, rows)], xbuf),
            (g_ref.at[0], gall.at[c]),
            (u_ref.at[0], uall.at[c]),
            (k_ref.at[:, heads], kvb.at[me, :, :key_dim]),
            (v_ref, kvb.at[me, :, key_dim:]),
            (d_ref.at[0, :, mine], dall.at[y, sublanes(c * units, units)]),
            (q_ref.at[:, heads], qb),
            (og_ref, ogb),
            (sg_ref, sgall.at[c]),
            (su_ref, suall.at[c]),
            (sd_ref.at[:, mine], sdall.at[y, sublanes(c * shared, shared)]),
            (mw_ref, mwb),
        )
        return pltpu.make_async_copy(*pairs[n], local.at[n])

    for n in range(12):
        load(n).start()

    barrier = pltpu.get_barrier_semaphore()

    def greet(ep, tp):
        pl.semaphore_signal(
            barrier, inc=1, device_id={"ep": ep, "tp": tp}, device_id_type=pl.DeviceIdType.MESH
        )

    for k in range(1, ep_count):
        greet(lax.rem(me + k, ep_count), j)
    greet(me, other_y)
    greet(me, buddy)

    bounds = []
    at = 0
    for size, only in splits:
        bounds.append((at, size, only))
        at += size

    def z_copy(zb, way, n):
        start, size, _ = bounds[n]
        ref = tok.at[zb * 2 + x, start : start + size]
        to = z + 1 - 2 * way
        return remote(ref, ref, z_send.at[way, zb, n], z_recv.at[zb, n], to * 2 + x, j)

    def x_copy(zb, column, n):
        start, size, only = bounds[n]
        ref = tok.at[zb * 2 + column, sublanes(start + y * only, size - only)]
        return remote(ref, ref, x_send.at[zb, n], x_recv.at[zb, n], across, j)

    def x_arrival(zb, n):
        start, size, only = bounds[n]
        ref = tok.at[zb * 2 + 1 - x, sublanes(start + y * only, size - only)]
        return remote(ref, ref, x_send.at[zb, n], x_recv.at[zb, n], across, j)

    def e_copy(zb, n):
        start, size, only = bounds[n]
        ref = tok.at[zb * 2 + 1 - x, sublanes(start + y * (size - only), only)]
        return remote(ref, ref, e_send.at[zb, n], e_recv.at[zb, n], me, other_y)

    def kz_copy(zb):
        ref = kvb.at[zb * 2 + x]
        return remote(ref, ref, kz_send.at[zb], kz_recv.at[zb], (z + 1) * 2 + x, j)

    def kx_copy(zb, column):
        ref = kvb.at[zb * 2 + column]
        return remote(ref, ref, kx_send.at[zb], kx_recv.at[zb], across, j)

    def s_copy(k):
        return remote(
            side.at[me], side.at[me], s_send.at[k - 1], s_recv.at[me], lax.rem(me + k, ep_count), j
        )

    def s_arrival(k):
        source = lax.rem(me + k, ep_count)
        return remote(
            side.at[source], side.at[source], s_send.at[k - 1], s_recv.at[source], source, j
        )

    def a_copy(block, team):
        ref = act.at[block, team]
        return remote(ref, ref, a_send.at[block], a_recv.at[block], me, other_y)

    def b_copy(core, n):
        pairs = (
            (g_ref.at[0], gall.at[core]),
            (u_ref.at[0], uall.at[core]),
            (sg_ref, sgall.at[core]),
            (su_ref, suall.at[core]),
            (d_ref.at[0, :, mine], dall.at[y, sublanes(core * units, units)]),
            (sd_ref.at[:, mine], sdall.at[y, sublanes(core * shared, shared)]),
        )
        return remote(*pairs[n], b_send.at[n], b_recv.at[n], me, buddy)

    def y_copy(team, n):
        pairs = (
            (d_ref.at[0, :, theirs], dall.at[team, sublanes(c * units, units)]),
            (sd_ref.at[:, theirs], sdall.at[team, sublanes(c * shared, shared)]),
            (sall.at[team], sall.at[team]),
        )
        return remote(*pairs[n], y_send.at[n], y_recv.at[n], me, other_y)

    def f_copy(core, n):
        refs = (
            dall.at[1 - y, sublanes(core * units, units)],
            sdall.at[1 - y, sublanes(core * shared, shared)],
        )
        return remote(refs[n], refs[n], f_send.at[n], f_recv.at[n], me, buddy)

    def xo_copy(zb, n):
        cols = pl.ds(n * piece, piece)
        return remote(
            res.at[zb * 2 + 1 - x, :, cols], xin.at[zb, :, cols],
            xo_send.at[zb, n], xo_recv.at[zb, n], across, j,
        )

    def zo_copy(zb, n):
        cols = pl.ds(n * piece, piece)
        return remote(
            zout.at[zb, :, cols], zin.at[z, :, cols],
            zo_send.at[zb, n], zo_recv.at[z, n], zb * 2 + x, j,
        )

    def zo_arrival(zb, n):
        cols = pl.ds(n * piece, piece)
        return remote(
            zout.at[zb, :, cols], zin.at[zb, :, cols],
            zo_send.at[zb, n], zo_recv.at[zb, n], zb * 2 + x, j,
        )

    def final(core, team, n):
        return eo_ref.at[
            sublanes(core * rows, rows), lanes(team * half + n * piece, piece)
        ]

    def ey_copy(team, n):
        ref = final(c, team, n)
        return remote(ref, ref, ey_send.at[n], ey_recv.at[n], me, other_y)

    def eb_copy(core, n):
        ref = final(core, y, n)
        return remote(ref, ref, eb_send.at[n], eb_recv.at[n], me, buddy)

    def ef_copy(core, n):
        ref = final(core, 1 - y, n)
        return remote(ref, ref, ef_send.at[n], ef_recv.at[n], me, buddy)

    def m_copy(core, n):
        ref = mo_ref.at[sublanes(core * part, part)]
        pairs = (
            (mpart.at[sublanes((1 - c) * part, part)], mpeer, buddy),
            (msum, mother, other_y),
            (ref, ref, buddy),
        )
        source, target, to = pairs[n]
        return remote(source, target, m_send.at[n], m_recv.at[n], me, to)

    at_row = lax.broadcasted_iota(jnp.int32, (length, length), 0)
    at_lane = lax.broadcasted_iota(jnp.int32, (length, length), 1)
    token_lanes = lanes(c * rows, rows)
    ids = ids_ref[:, token_lanes]
    route = rw_ref[:, token_lanes]
    for e in range(ep_count):
        side[me, e : e + 1, :] = jnp.sum(jnp.where(ids == e, route, 0.0), axis=0, keepdims=True)
    forget = fg_ref[pl.ds(y, 1), :]
    small = jnp.exp(-jnp.abs(forget))
    kept = jnp.minimum(forget, 0.0) - jnp.log1p(small)
    kept_column = jnp.sum(jnp.where(at_row == at_lane, kept, 0.0), axis=1, keepdims=True)
    cumulative = jnp.sum(jnp.where(at_row <= at_lane, kept_column, 0.0), axis=0, keepdims=True)
    side[me, ep_count : ep_count + 1, :] = ig_ref[pl.ds(y, 1), :] - cumulative
    side[me, ep_count + 1 : ep_count + 2, :] = jnp.broadcast_to(
        jnp.sum(kept, axis=1, keepdims=True), (1, length)
    )

    def normalize(start, size):
        def group(n, carry):
            at_rows = sublanes(start + n * 16, 16)
            wide_rows = xbuf[at_rows, :].astype(wide)
            scale = lax.rsqrt(jnp.mean(wide_rows * wide_rows, axis=1, keepdims=True) + epsilon)
            tok[me, at_rows, :] = (wide_rows * scale * gain_ref[...]).astype(low)
            return carry

        lax.fori_loop(0, size // 16, group, 0)

    def can_go(way):
        to = z + 1 - 2 * way
        return (to >= 0) & (to < lines)

    load(0).wait()
    normalize(bounds[0][0], bounds[0][1])
    pl.semaphore_wait(barrier, ep_count + 1)
    for n in range(len(bounds)):
        if n:
            normalize(bounds[n][0], bounds[n][1])
        for way in range(2):

            @pl.when(can_go(way))
            def _():
                z_copy(z, way, n).start()

        x_copy(z, x, n).start()
        if n == 0:
            for i in range(6):
                b_copy(c, i).start()
            y_copy(y, 0).start()
    for k in range(1, ep_count):
        s_copy(k).start()
    load(3).wait()
    load(4).wait()

    @pl.when(z + 1 < lines)
    def _():
        kz_copy(z).start()

    @pl.when(x == 0)
    def _():
        kx_copy(z, x).start()

    load(1).wait()
    load(2).wait()
    b_copy(1 - c, 0).wait_recv()
    b_copy(1 - c, 1).wait_recv()

    def activate(block):
        for h in range(2):
            gate = jnp.dot(tok[block], gall[h], preferred_element_type=wide)
            up = jnp.dot(tok[block], uall[h], preferred_element_type=wide)
            act[block, y, :, h * units : (h + 1) * units] = (
                gate / (1.0 + jnp.exp(-gate)) * up
            ).astype(low)
        a_copy(block, y).start()

    def valid(s, d, zb):
        return (s >= 0) & (s < lines) & (zb >= 0) & (zb < lines) & ((s > 0) | (d == 0))

    def both_ways(s, work):
        def one(d, carry):
            zb = z + s * (2 * d - 1)

            @pl.when(valid(s, d, zb))
            def _():
                work(d, zb)

            return carry

        lax.fori_loop(0, 2, one, 0)

    def forward(d, zb):
        for n in range(len(bounds)):
            z_copy(zb, d, n).wait_recv()

            @pl.when(can_go(d))
            def _():
                z_copy(zb, d, n).start()

            x_copy(zb, x, n).start()

        @pl.when(d == 0)
        def _():
            kz_copy(zb).wait_recv()

            @pl.when(z + 1 < lines)
            def _():
                kz_copy(zb).start()

            kx_copy(zb, x).start()

    def pass_on(d, zb):
        for n in range(len(bounds)):
            x_arrival(zb, n).wait_recv()
            if bounds[n][2]:
                e_copy(zb, n).start()

    def near(d, zb):
        activate(zb * 2 + x)

    def far(d, zb):
        for n in range(len(bounds)):
            if bounds[n][2]:
                e_copy(zb, n).wait_recv()
        activate(zb * 2 + 1 - x)

    def finish(block):
        a_copy(block, 1 - y).wait_recv()
        weight = jnp.sum(
            jnp.where(at_row == at_lane, side[block, pl.ds(me, 1), :], 0.0), axis=1, keepdims=True
        )
        for n in range(halves):
            cols = slice(n * piece, (n + 1) * piece)
            total = jnp.dot(act[block, 0], dall[0, :, cols], preferred_element_type=wide)
            total += jnp.dot(act[block, 1], dall[1, :, cols], preferred_element_type=wide)
            res[block, :, cols] = (total * weight).astype(low)

    def finish_near(d, zb):
        finish(zb * 2 + x)

    def finish_far(d, zb):
        finish(zb * 2 + 1 - x)
        for n in range(halves):
            xo_copy(zb, n).start()

    def send_home(d, zb):
        for n in range(halves):
            cols = slice(n * piece, (n + 1) * piece)
            xo_copy(zb, n).wait_recv()
            zout[zb, :, cols] = (
                res[zb * 2 + x, :, cols].astype(wide) + xin[zb, :, cols].astype(wide)
            ).astype(low)
            zo_copy(zb, n).start()

    def memory(d, zb):
        @pl.when((d == 0) & (zb * 2 + 1 - x < me))
        def _():
            kx_copy(zb, 1 - x).wait_recv()

        def one(n, carry):
            block = zb * 2 + n

            @pl.when((d == 0) & (block <= me))
            def _():
                scores = lax.dot_general(
                    qb[...], kvb[block, :, :key_dim], (((1,), (1,)), ((), ())),
                    preferred_element_type=wide,
                ) * (key_dim ** -0.5)
                seen = (block < me) | (at_row >= at_lane)
                shown = jnp.where(seen, brow[block, 0:1, :] - stab[...], lowest)
                weights = jnp.where(seen, scores * jnp.exp(shown), 0.0)
                num[...] += jnp.dot(
                    weights.astype(low), kvb[block, :, key_dim:], preferred_element_type=wide
                )
                den[...] += jnp.broadcast_to(
                    jnp.sum(weights, axis=1, keepdims=True), den.shape
                )

            return carry

        lax.fori_loop(0, 2, one, 0)

    def prepare():
        for k in range(1, ep_count):
            s_arrival(k).wait_recv()
        gap = jnp.zeros((1, length), wide)
        top = jnp.full((1, length), lowest, wide)
        for b in reversed(range(ep_count)):
            earlier = b < me
            gap = jnp.where(earlier, gap + side[b, ep_count + 1 : ep_count + 2, :], gap)
            row = side[b, ep_count : ep_count + 1, :] + gap
            brow[b, 0:1, :] = row
            top = jnp.where(earlier, jnp.maximum(top, row), top)
        own = side[me, ep_count : ep_count + 1, :]
        within = jnp.max(
            jnp.where(at_row >= at_lane, own, lowest), axis=1, keepdims=True
        )
        before = jnp.max(jnp.maximum(top, gap), axis=1, keepdims=True)
        stab[...] = jnp.broadcast_to(jnp.maximum(within, before), stab.shape)
        num[...] = jnp.zeros_like(num)
        den[...] = jnp.zeros_like(den)
        load(6).wait()
        load(8).wait()
        load(9).wait()
        for n in (2, 3):
            b_copy(1 - c, n).wait_recv()
        for h in range(2):
            gate = jnp.dot(tok[me], sgall[h], preferred_element_type=wide)
            up = jnp.dot(tok[me], suall[h], preferred_element_type=wide)
            sall[y, :, h * shared : (h + 1) * shared] = (
                gate / (1.0 + jnp.exp(-gate)) * up
            ).astype(low)
        for n in (1, 2):
            y_copy(y, n).start()
        load(5).wait()
        y_copy(1 - y, 0).wait_recv()
        f_copy(c, 0).start()
        b_copy(1 - c, 4).wait_recv()
        f_copy(1 - c, 0).wait_recv()

    def step(t, carry):
        both_ways(jnp.where(t > 0, t, lines), forward)
        both_ways(jnp.where(t > 2, t - 2, lines), finish_far)
        both_ways(t - 1, pass_on)
        both_ways(t, near)
        both_ways(jnp.where(t > 3, t - 3, lines), send_home)
        both_ways(t - 1, far)

        @pl.when(t == 1)
        def _():
            prepare()

        both_ways(t - 1, memory)
        both_ways(t - 1, finish_near)
        return carry

    lax.fori_loop(0, lines + 1, step, 0)

    def late(n, carry):
        both_ways(jnp.where(n == 0, lines - 1, 0), finish_far)

        @pl.when(n == 0)
        def _():
            both_ways(lines - 2, send_home)

        return carry

    lax.fori_loop(0, 2, late, 0)

    load(7).wait()
    load(11).wait()
    hidden = num[...] / jnp.maximum(jnp.abs(den[:, 0:1]), den_floor)
    gated = (hidden * (1.0 / (1.0 + jnp.exp(-ogb[...].astype(wide))))).astype(low)
    for n in range(4):
        cols = slice(n * half // 2, (n + 1) * half // 2)
        mpart[:, cols] = jnp.dot(gated, mwb[:, cols], preferred_element_type=wide).astype(low)
    m_copy(c, 0).start()
    load(10).wait()
    y_copy(1 - y, 1).wait_recv()
    f_copy(c, 1).start()
    y_copy(1 - y, 2).wait_recv()
    b_copy(1 - c, 5).wait_recv()
    m_copy(c, 0).wait_recv()
    msum[...] = (
        mpart[sublanes(c * part, part), :].astype(wide) + mpeer[...].astype(wide)
    ).astype(low)
    m_copy(c, 1).start()
    both_ways(lines - 1, send_home)
    f_copy(1 - c, 1).wait_recv()
    m_copy(c, 1).wait_recv()
    mo_ref[sublanes(c * part, part), :] = (
        msum[...].astype(wide) + mother[...].astype(wide)
    ).astype(low)
    m_copy(c, 2).start()

    for n in range(halves):
        cols = slice(n * piece, (n + 1) * piece)
        xo_copy(z, n).wait_recv()
        total = res[me, :, cols].astype(wide) + xin[z, :, cols].astype(wide)
        for team in range(2):
            total += jnp.dot(sall[team], sdall[team, :, cols], preferred_element_type=wide)
        for k in range(1, lines):
            source = lax.rem(z + k, lines)
            zo_arrival(source, n).wait_recv()
            total += zin[source, :, cols].astype(wide)
        eo_ref[sublanes(c * rows, rows), lanes(y * half + n * piece, piece)] = total.astype(low)
        ey_copy(y, n).start()
        eb_copy(c, n).start()
    for n in range(halves):
        ey_copy(1 - y, n).wait_recv()
        ef_copy(c, n).start()
    m_copy(1 - c, 2).wait_recv()
    for n in range(halves):
        eb_copy(1 - c, n).wait_recv()
        ef_copy(1 - c, n).wait_recv()

    for n in range(6):
        b_copy(c, n).wait_send()
    for n in range(3):
        y_copy(y, n).wait_send()
        m_copy(c, n).wait_send()
    for n in range(2):
        f_copy(c, n).wait_send()
    for n in range(halves):
        ey_copy(y, n).wait_send()
        eb_copy(c, n).wait_send()
        ef_copy(c, n).wait_send()
    for k in range(1, ep_count):
        s_copy(k).wait_send()

    @pl.when(x == 0)
    def _():
        kx_copy(z, x).wait_send()

    def drain(zb, carry):
        for way in range(2):
            passing = (zb <= z) if way == 0 else (zb >= z)

            @pl.when(can_go(way) & passing)
            def _():
                for n in range(len(bounds)):
                    z_copy(zb, way, n).wait_send()

        @pl.when((z + 1 < lines) & (zb <= z))
        def _():
            kz_copy(zb).wait_send()

        @pl.when(zb < z)
        def _():
            kx_copy(zb, x).wait_send()

        for n in range(len(bounds)):
            x_copy(zb, x, n).wait_send()
            if bounds[n][2]:
                e_copy(zb, n).wait_send()
        for n in range(halves):
            xo_copy(zb, n).wait_send()

            @pl.when(zb != z)
            def _():
                zo_copy(zb, n).wait_send()

        for n in range(2):
            a_copy(zb * 2 + n, y).wait_send()
        return carry

    lax.fori_loop(0, lines, drain, 0)


def lane_program(
    queries, key_vectors, values, out_gate, input_gate, forget_gate, mix_weight,
    expert_input, norm_gain, route_ids, route_weights, expert_gate, expert_up, expert_down,
    shared_gate, shared_up, shared_down,
):
    ep_count = lax.axis_size("ep")
    lines = ep_count // 2
    tokens, width = expert_input.shape
    rows, half = tokens // 2, width // 2
    length, channels = values.shape
    units, shared = expert_gate.shape[2], shared_gate.shape[1]
    low, wide, dma = jnp.bfloat16, jnp.float32, pltpu.SemaphoreType.DMA
    side_rows = ep_count + 2 + -(ep_count + 2) % 8
    chunks = len(splits)
    vmem = pl.BlockSpec(memory_space=pltpu.VMEM)
    hbm = pl.BlockSpec(memory_space=pl.ANY)

    def buffer(*shape, dtype=low):
        return pltpu.VMEM(shape, dtype)

    return pl.pallas_call(
        functools.partial(lane_kernel, lines),
        out_shape=(
            jax.ShapeDtypeStruct((length, width), low),
            jax.ShapeDtypeStruct((tokens, width), low),
        ),
        in_specs=[vmem] * 5 + [hbm] * 12,
        out_specs=(vmem, vmem),
        scratch_shapes=[
            buffer(rows, width),
            buffer(length, KEY_DIM),
            buffer(length, channels),
            buffer(channels, width),
            buffer(2, width, units),
            buffer(2, width, units),
            buffer(2, 2 * units, half),
            buffer(2, width, shared),
            buffer(2, width, shared),
            buffer(2, 2 * shared, half),
            buffer(2, rows, 2 * shared),
            buffer(ep_count, rows, width),
            buffer(ep_count, 2, rows, 2 * units),
            buffer(ep_count, length, KEY_DIM + channels),
            buffer(ep_count, side_rows, rows, dtype=wide),
            buffer(ep_count, 8, length, dtype=wide),
            buffer(length, length, dtype=wide),
            buffer(length, channels, dtype=wide),
            buffer(length, 128, dtype=wide),
            buffer(ep_count, rows, half),
            buffer(lines, rows, half),
            buffer(lines, rows, half),
            buffer(lines, rows, half),
            buffer(length, width),
            buffer(length // 2, width),
            buffer(length // 2, width),
            buffer(length // 2, width),
            dma((12,)),
            dma((2, lines, chunks)), dma((lines, chunks)),
            dma((lines, chunks)), dma((lines, chunks)),
            dma((lines, chunks)), dma((lines, chunks)),
            dma((lines,)), dma((lines,)), dma((lines,)), dma((lines,)),
            dma((ep_count - 1,)), dma((ep_count,)),
            dma((ep_count,)), dma((ep_count,)),
            dma((6,)), dma((6,)), dma((3,)), dma((3,)), dma((2,)), dma((2,)),
            dma((lines, halves)), dma((lines, halves)),
            dma((lines, halves)), dma((lines, halves)),
            dma((halves,)), dma((halves,)), dma((halves,)), dma((halves,)),
            dma((halves,)), dma((halves,)),
            dma((3,)), dma((3,)),
        ],
        compiler_params=pltpu.CompilerParams(
            collective_id=0, has_side_effects=True, vmem_limit_bytes=56 * 1024 * 1024
        ),
    )(
        input_gate.T, forget_gate.T, norm_gain[None, :], route_ids.T, route_weights.T,
        queries, key_vectors, values, out_gate, mix_weight, expert_input,
        expert_gate, expert_up, expert_down, shared_gate, shared_up, shared_down,
    )


def expert_half(
    expert_input,
    norm_gain,
    route_ids,
    route_weights,
    expert_gate,
    expert_up,
    expert_down,
    shared_gate,
    shared_up,
    shared_down,
):
    ep_count = lax.axis_size("ep")
    tp_count = lax.axis_size("tp")
    tp_rank = lax.axis_index("tp")
    tokens = expert_input.shape[0]
    top_count = route_ids.shape[1]
    slice_units = expert_gate.shape[2]
    group_size = FF // slice_units
    per_ep = tp_count // group_size
    team_index = tp_rank // group_size
    expert_count = ep_count * per_ep
    capacity = 2 * tokens * top_count // expert_count
    rows_wide = expert_input.astype(jnp.float32)
    normed = (
        rows_wide
        * lax.rsqrt(jnp.mean(rows_wide * rows_wide, axis=-1, keepdims=True) + epsilon)
        * norm_gain
    ).astype(jnp.bfloat16)
    chosen = route_ids.reshape(-1)
    onehot = (chosen[:, None] == jnp.arange(expert_count, dtype=jnp.int32)[None, :]).astype(
        jnp.int32
    )
    slot_rank = jnp.sum((jnp.cumsum(onehot, axis=0) - onehot) * onehot, axis=1)
    in_team = chosen % per_ep == team_index
    target = jnp.where(in_team, chosen // per_ep * capacity + slot_rank, ep_count * capacity)
    token_of = jnp.arange(chosen.shape[0], dtype=jnp.int32) // top_count
    slot_token = jnp.zeros((ep_count * capacity,), jnp.int32).at[target].set(token_of, mode="drop")
    slot_live = jnp.zeros((ep_count * capacity,), jnp.int32).at[target].set(1, mode="drop")
    outgoing = jnp.where(slot_live[:, None] > 0, normed[slot_token], jnp.zeros((), jnp.bfloat16))
    outgoing = outgoing.reshape(ep_count, capacity, D)
    gate_slice = expert_gate[0]
    up_slice = expert_up[0]
    down_slice = expert_down[0]
    arrived = lax.all_to_all(outgoing, "ep", split_axis=0, concat_axis=0, tiled=True)
    gate_val = jnp.einsum("sid,df->sif", arrived, gate_slice, preferred_element_type=jnp.float32)
    up_val = jnp.einsum("sid,df->sif", arrived, up_slice, preferred_element_type=jnp.float32)
    hidden = (jax.nn.silu(gate_val) * up_val).astype(jnp.bfloat16)
    partial_value = jnp.einsum(
        "sif,fd->sid", hidden, down_slice, preferred_element_type=jnp.float32
    )
    partial_value = partial_value.astype(jnp.bfloat16)
    returned = lax.all_to_all(partial_value, "ep", split_axis=0, concat_axis=0, tiled=True)
    flat_back = returned.reshape(ep_count * capacity, returned.shape[2])
    gather_at = jnp.where(in_team, target, 0).reshape(tokens, top_count)
    weight_at = jnp.where(in_team, route_weights.reshape(-1), 0.0).reshape(tokens, top_count)
    combined = jnp.zeros((tokens, returned.shape[2]), jnp.float32)
    for pick_index in range(top_count):
        combined = (
            combined
            + flat_back[gather_at[:, pick_index]].astype(jnp.float32)
            * weight_at[:, pick_index][:, None]
        )
    shared_gate_val = jnp.dot(normed, shared_gate, preferred_element_type=jnp.float32)
    shared_up_val = jnp.dot(normed, shared_up, preferred_element_type=jnp.float32)
    shared_act = (jax.nn.silu(shared_gate_val) * shared_up_val).astype(jnp.bfloat16)
    return combined + jnp.dot(shared_act, shared_down, preferred_element_type=jnp.float32)


def shards(
    queries,
    key_vectors,
    values,
    out_gate,
    input_gate,
    forget_gate,
    mix_weight,
    expert_input,
    norm_gain,
    route_ids,
    route_weights,
    expert_gate,
    expert_up,
    expert_down,
    shared_gate,
    shared_up,
    shared_down,
):
    ep_count, tp_count = lax.axis_size("ep"), lax.axis_size("tp")
    tokens, slots = expert_input.shape[0], route_ids.shape[1] * 2 * expert_input.shape[0]
    per_ep = tp_count * expert_gate.shape[2] // FF
    even = ep_count % 2 == 0 and tp_count == 4 and MEMORY_HEADS * 2 == tp_count
    blocked = values.shape[0] == BLOCK and tokens == 2 * BLOCK and ep_count > 2
    dense = even and blocked and per_ep == 1 and slots // (ep_count * per_ep) >= tokens
    experts = (
        expert_input,
        norm_gain,
        route_ids,
        route_weights,
        expert_gate,
        expert_up,
        expert_down,
        shared_gate,
        shared_up,
        shared_down,
    )
    if dense:
        return lane_program(
            queries, key_vectors, values, out_gate, input_gate, forget_gate, mix_weight, *experts
        )
    query_head, both, gates = mixer_local(
        queries, key_vectors, values, input_gate, forget_gate
    )
    both = lax.all_gather(both, "ep", axis=0, tiled=True)
    gates = lax.all_gather(gates, "ep", axis=1, tiled=True)
    gated_rows = mixer_rows(query_head, both, gates, out_gate)
    mixer_partial = jnp.dot(gated_rows, mix_weight, preferred_element_type=jnp.float32)
    expert_partial = expert_half(*experts)
    mixer_piece = lax.psum_scatter(
        mixer_partial.astype(jnp.bfloat16), "tp", scatter_dimension=0, tiled=True
    )
    mixer_out = lax.all_gather(mixer_piece, "tp", axis=0, tiled=True)
    expert_piece = lax.psum_scatter(expert_partial, "tp", scatter_dimension=0, tiled=True).astype(
        jnp.bfloat16
    )
    expert_out = lax.all_gather(expert_piece, "tp", axis=0, tiled=True)
    return (mixer_out, expert_out)


def solution(mesh):
    return jax.shard_map(
        shards,
        mesh=mesh,
        in_specs=(
            P("ep", None),
            P("ep", None),
            P("ep", "tp"),
            P("ep", "tp"),
            P("ep", None),
            P("ep", None),
            P("tp", None),
            P("ep", None),
            P(),
            P("ep", None),
            P("ep", None),
            P(("ep", "tp"), None, None),
            P(("ep", "tp"), None, None),
            P(("ep", "tp"), None, None),
            P(None, "tp"),
            P(None, "tp"),
            P("tp", None),
        ),
        out_specs=(P("ep", None), P("ep", None)),
        check_vma=False,
    )
```

```python
import functools

import jax
import jax.numpy as jnp
from jax import lax
from jax.experimental import pallas as pl
from jax.experimental.pallas import tpu as pltpu
from jax.sharding import PartitionSpec as P

D = 2048
MEMORY_HEADS = 2
KEY_DIM = 256
BLOCK = 128
FF = 1024


epsilon = 1e-06
lowest = -1e30
den_floor = 4.0


def mixer_local(queries, key_vectors, values, input_gate, forget_gate):
    tp_count = lax.axis_size("tp")
    tp_rank = lax.axis_index("tp")
    head_index = tp_rank // (tp_count // MEMORY_HEADS)
    offset = head_index * KEY_DIM
    query_head = lax.dynamic_slice_in_dim(queries, offset, KEY_DIM, 1)
    key_head = lax.dynamic_slice_in_dim(key_vectors, offset, KEY_DIM, 1)
    select = jnp.arange(MEMORY_HEADS, dtype=jnp.int32)[None, :] == head_index
    gates = jnp.stack(
        [
            jnp.sum(jnp.where(select, input_gate, 0.0), axis=1),
            jax.nn.log_sigmoid(jnp.sum(jnp.where(select, forget_gate, 0.0), axis=1)),
        ]
    )
    return query_head, jnp.concatenate([key_head, values], axis=1), gates


def mixer_rows(query_head, both, gates, out_gate):
    ep_count = lax.axis_size("ep")
    ep_rank = lax.axis_index("ep")
    length = query_head.shape[0]
    factor = KEY_DIM ** (-0.5)
    keys_all = both[:, :KEY_DIM]
    values_all = both[:, KEY_DIM:]
    total = ep_count * length
    blocks = total // BLOCK
    mine = length // BLOCK
    input_all = gates[0].reshape(blocks, BLOCK)
    cumulative = jnp.cumsum(gates[1].reshape(blocks, BLOCK), axis=1)
    block_total = cumulative[:, -1]
    index = jnp.arange(blocks, dtype=jnp.int32)
    here = ep_rank * mine + jnp.arange(mine, dtype=jnp.int32)
    between = (index[None, None, :] > index[None, :, None]) & (
        index[None, None, :] < here[:, None, None]
    )
    gap = jnp.sum(jnp.where(between, block_total[None, None, :], 0.0), axis=2)
    ahead = jnp.sum(jnp.where(index[None, :] < here[:, None], block_total[None, :], 0.0), axis=1)
    keep = block_total[:, None] - cumulative + input_all
    own_cumulative = lax.dynamic_slice_in_dim(cumulative, ep_rank * mine, mine, 0)
    same = index[None, :] == here[:, None]
    column = jnp.where(same[:, :, None], input_all - cumulative, keep + gap[:, :, None])
    log_weight = own_cumulative[:, :, None, None] + column[:, None]
    row_at = jnp.arange(BLOCK, dtype=jnp.int32)
    visible = (index[None, :] < here[:, None])[:, None, :, None] | (
        same[:, None, :, None] & (row_at[None, :, None, None] >= row_at[None, None, None, :])
    )
    log_weight = jnp.where(visible, log_weight, -jnp.inf).reshape(length, total)
    carried = (own_cumulative + ahead[:, None]).reshape(length)
    stabilizer = jnp.maximum(carried, jnp.max(log_weight, axis=1))
    within = jnp.exp(log_weight - stabilizer[:, None])
    scores = (
        jnp.einsum("td,sd->ts", query_head, keys_all, preferred_element_type=jnp.float32) * factor
    )
    weights = scores * within
    numerator = jnp.dot(
        weights.astype(jnp.bfloat16), values_all, preferred_element_type=jnp.float32
    )
    denominator = jnp.sum(weights, axis=1)
    hidden = numerator / jnp.maximum(jnp.abs(denominator), den_floor)[:, None]
    gated_rows = (hidden * jax.nn.sigmoid(out_gate.astype(jnp.float32))).astype(jnp.bfloat16)
    return gated_rows


chunks = 2
alone = 16
halves = 2
kinds = 18
(
    FORWARD, KEYS, PASS, ACTIVATE, FINISH, HOME, MEMORY, DOWN, OWN_KEYS,
    SHARED, SHARED_DOWN, TEAM, TEAM_DONE, PROJECT, PAIR, PROJECTED, SHARED_TEAM, LAST,
) = range(kinds)
PLANS = {
    4: (
        (
            224, 256, 97, 8, 288, 65, 9, 352, 104, 72, 16, 384, 73, 136, 128, 17,
            129, 64, 108, 80, 24, 81, 116, 25, 112, 192, 88, 416, 120, 148, 149, 89,
            140, 141, 137, 100, 144, 145, 176, 177, 124, 152, 168, 448, 169, 156, 153, 157,
            320, 184, 132, 133, 185, 512, 544, 545, 480,
        ),
        (
            224, 16, 0, 288, 105, 17, 112, 80, 1, 352, 384, 96, 136, 24, 73, 81,
            25, 128, 137, 256, 144, 64, 32, 65, 145, 116, 88, 100, 89, 72, 148, 149,
            120, 132, 133, 124, 108, 176, 192, 320, 200, 416, 156, 157, 152, 160, 140, 129,
            448, 184, 161, 512, 141, 177, 153, 185, 544, 545, 480,
        ),
        (
            224, 24, 80, 8, 113, 9, 25, 81, 120, 352, 384, 104, 0, 72, 73, 88,
            1, 96, 89, 136, 108, 40, 124, 152, 153, 32, 64, 288, 140, 65, 137, 116,
            256, 141, 156, 157, 100, 128, 129, 168, 320, 208, 200, 169, 192, 132, 133, 184,
            416, 448, 185, 148, 160, 512, 149, 161, 144, 145, 544, 480, 545,
        ),
        (
            224, 121, 16, 288, 17, 112, 256, 88, 80, 8, 81, 9, 352, 72, 116, 0,
            73, 104, 384, 144, 148, 108, 1, 96, 145, 136, 40, 89, 152, 176, 140, 141,
            32, 64, 65, 153, 124, 128, 100, 48, 149, 168, 200, 137, 320, 169, 216, 192,
            132, 133, 208, 416, 177, 448, 160, 156, 157, 129, 161, 512, 544, 545, 480,
        ),
    ),
}


def lane_kernel(
    lines, plan,
    ig_ref, fg_ref, gain_ref, ids_ref, rw_ref,
    q_ref, k_ref, v_ref, og_ref, mw_ref, x_ref, g_ref, u_ref, d_ref, sg_ref, su_ref, sd_ref,
    mo_ref, eo_ref,
    xbuf, qb, ogb, mwb, gall, uall, dall, sgall, suall, sdall, sall,
    tok, act, kvb, side, brow, stab, num, den, res, xin, zout, zin, mpart, mpeer, msum, mother,
    local, z_send, z_recv, x_send, x_recv, e_send, e_recv, kz_send, kz_recv, kx_send, kx_recv,
    s_send, s_recv, a_send, a_recv, b_send, b_recv, y_send, y_recv, f_send, f_recv,
    xo_send, xo_recv, zo_send, zo_recv, ey_send, ey_recv, eb_send, eb_recv, ef_send, ef_recv,
    m_send, m_recv,
):
    me = lax.axis_index("ep")
    j = lax.axis_index("tp")
    z, x = me // 2, me % 2
    y, c = j // 2, j % 2
    ep_count = 2 * lines
    rows = x_ref.shape[0] // 2
    length = q_ref.shape[0]
    key_dim = qb.shape[1]
    half = dall.shape[2]
    units = g_ref.shape[2]
    shared = sg_ref.shape[1]
    piece = half // halves
    part = length // 2
    low, wide = jnp.bfloat16, jnp.float32

    def remote(src, dst, send, recv, ep, tp):
        return pltpu.make_async_remote_copy(
            src_ref=src, dst_ref=dst, send_sem=send, recv_sem=recv,
            device_id={"ep": ep, "tp": tp}, device_id_type=pl.DeviceIdType.MESH,
        )

    across = z * 2 + 1 - x
    other_y = (1 - y) * 2 + c
    buddy = y * 2 + 1 - c

    def lanes(start, size):
        return pl.ds(pl.multiple_of(start, 128), size)

    def sublanes(start, size):
        return pl.ds(pl.multiple_of(start, 8), size)

    mine = lanes(y * half, half)
    theirs = lanes((1 - y) * half, half)
    heads = lanes(y * key_dim, key_dim)

    def load(n):
        pairs = (
            (x_ref.at[sublanes(c * rows, rows)], xbuf),
            (g_ref.at[0], gall.at[c]),
            (u_ref.at[0], uall.at[c]),
            (k_ref.at[:, heads], kvb.at[me, :, :key_dim]),
            (v_ref, kvb.at[me, :, key_dim:]),
            (d_ref.at[0, :, mine], dall.at[y, sublanes(c * units, units)]),
            (q_ref.at[:, heads], qb),
            (og_ref, ogb),
            (sg_ref, sgall.at[c]),
            (su_ref, suall.at[c]),
            (sd_ref.at[:, mine], sdall.at[y, sublanes(c * shared, shared)]),
            (mw_ref, mwb),
        )
        return pltpu.make_async_copy(*pairs[n], local.at[n])

    for n in range(12):
        load(n).start()

    barrier = pltpu.get_barrier_semaphore()

    def greet(ep, tp):
        pl.semaphore_signal(
            barrier, inc=1, device_id={"ep": ep, "tp": tp}, device_id_type=pl.DeviceIdType.MESH
        )

    for k in range(1, ep_count):
        greet(lax.rem(me + k, ep_count), j)
    greet(me, other_y)
    greet(me, buddy)

    chunk = rows // chunks

    def z_copy(zb, way, n):
        ref = tok.at[zb * 2 + x, sublanes(n * chunk, chunk)]
        to = z + 1 - 2 * way
        return remote(ref, ref, z_send.at[way, zb, n], z_recv.at[zb, n], to * 2 + x, j)

    def x_copy(zb, column, n):
        ref = tok.at[zb * 2 + column, sublanes(n * chunk + y * alone, chunk - alone)]
        return remote(ref, ref, x_send.at[zb, n], x_recv.at[zb, n], across, j)

    def e_copy(zb, n):
        ref = tok.at[zb * 2 + 1 - x, sublanes(n * chunk + y * (chunk - alone), alone)]
        return remote(ref, ref, e_send.at[zb, n], e_recv.at[zb, n], me, other_y)

    def kz_copy(zb):
        ref = kvb.at[zb * 2 + x]
        return remote(ref, ref, kz_send.at[zb], kz_recv.at[zb], (z + 1) * 2 + x, j)

    def kx_copy(zb, column):
        ref = kvb.at[zb * 2 + column]
        return remote(ref, ref, kx_send.at[zb], kx_recv.at[zb], across, j)

    def s_copy(k):
        return remote(
            side.at[me], side.at[me], s_send.at[k - 1], s_recv.at[me], lax.rem(me + k, ep_count), j
        )

    def s_arrival(k):
        source = lax.rem(me + k, ep_count)
        return remote(
            side.at[source], side.at[source], s_send.at[k - 1], s_recv.at[source], source, j
        )

    def a_copy(block, team):
        ref = act.at[block, team]
        return remote(ref, ref, a_send.at[block], a_recv.at[block], me, other_y)

    def b_copy(core, n):
        pairs = (
            (g_ref.at[0], gall.at[core]),
            (u_ref.at[0], uall.at[core]),
            (sg_ref, sgall.at[core]),
            (su_ref, suall.at[core]),
            (d_ref.at[0, :, mine], dall.at[y, sublanes(core * units, units)]),
            (sd_ref.at[:, mine], sdall.at[y, sublanes(core * shared, shared)]),
        )
        return remote(*pairs[n], b_send.at[n], b_recv.at[n], me, buddy)

    def y_copy(team, n):
        pairs = (
            (d_ref.at[0, :, theirs], dall.at[team, sublanes(c * units, units)]),
            (sd_ref.at[:, theirs], sdall.at[team, sublanes(c * shared, shared)]),
            (sall.at[team], sall.at[team]),
        )
        return remote(*pairs[n], y_send.at[n], y_recv.at[n], me, other_y)

    def f_copy(core, n):
        refs = (
            dall.at[1 - y, sublanes(core * units, units)],
            sdall.at[1 - y, sublanes(core * shared, shared)],
        )
        return remote(refs[n], refs[n], f_send.at[n], f_recv.at[n], me, buddy)

    def xo_copy(zb, n):
        cols = lanes(n * piece, piece)
        return remote(
            res.at[zb * 2 + 1 - x, :, cols], xin.at[zb, :, cols],
            xo_send.at[zb, n], xo_recv.at[zb, n], across, j,
        )

    def zo_copy(zb, n):
        cols = lanes(n * piece, piece)
        return remote(
            zout.at[zb, :, cols], zin.at[z, :, cols],
            zo_send.at[zb, n], zo_recv.at[z, n], zb * 2 + x, j,
        )

    def zo_arrival(zb, n):
        cols = lanes(n * piece, piece)
        return remote(
            zout.at[zb, :, cols], zin.at[zb, :, cols],
            zo_send.at[zb, n], zo_recv.at[zb, n], zb * 2 + x, j,
        )

    def final(core, team, n):
        return eo_ref.at[
            sublanes(core * rows, rows), lanes(team * half + n * piece, piece)
        ]

    def ey_copy(team, n):
        ref = final(c, team, n)
        return remote(ref, ref, ey_send.at[n], ey_recv.at[n], me, other_y)

    def eb_copy(core, n):
        ref = final(core, y, n)
        return remote(ref, ref, eb_send.at[n], eb_recv.at[n], me, buddy)

    def ef_copy(core, n):
        ref = final(core, 1 - y, n)
        return remote(ref, ref, ef_send.at[n], ef_recv.at[n], me, buddy)

    def m_copy(core, n):
        ref = mo_ref.at[sublanes(core * part, part)]
        pairs = (
            (mpart.at[sublanes((1 - c) * part, part)], mpeer, buddy),
            (msum, mother, other_y),
            (ref, ref, buddy),
        )
        source, target, to = pairs[n]
        return remote(source, target, m_send.at[n], m_recv.at[n], me, to)

    at_row = lax.broadcasted_iota(jnp.int32, (length, length), 0)
    at_lane = lax.broadcasted_iota(jnp.int32, (length, length), 1)
    token_lanes = lanes(c * rows, rows)
    ids = ids_ref[:, token_lanes]
    route = rw_ref[:, token_lanes]
    for e in range(ep_count):
        side[me, e : e + 1, :] = jnp.sum(jnp.where(ids == e, route, 0.0), axis=0, keepdims=True)
    forget = fg_ref[pl.ds(y, 1), :]
    small = jnp.exp(-jnp.abs(forget))
    kept = jnp.minimum(forget, 0.0) - jnp.log1p(small)
    kept_column = jnp.sum(jnp.where(at_row == at_lane, kept, 0.0), axis=1, keepdims=True)
    cumulative = jnp.sum(jnp.where(at_row <= at_lane, kept_column, 0.0), axis=0, keepdims=True)
    side[me, ep_count : ep_count + 1, :] = ig_ref[pl.ds(y, 1), :] - cumulative
    side[me, ep_count + 1 : ep_count + 2, :] = jnp.broadcast_to(
        jnp.sum(kept, axis=1, keepdims=True), (1, length)
    )

    def normalize(n):
        def group(i, carry):
            at_rows = sublanes(n * chunk + i * 16, 16)
            wide_rows = xbuf[at_rows, :].astype(wide)
            scale = lax.rsqrt(jnp.mean(wide_rows * wide_rows, axis=1, keepdims=True) + epsilon)
            tok[me, at_rows, :] = (wide_rows * scale * gain_ref[...]).astype(low)
            return carry

        lax.fori_loop(0, chunk // 16, group, 0)

    def can_go(way):
        to = z + 1 - 2 * way
        return (to >= 0) & (to < lines)

    load(0).wait()
    normalize(0)
    pl.semaphore_wait(barrier, ep_count + 1)
    for n in range(chunks):
        if n:
            normalize(n)
        for way in range(2):

            @pl.when(can_go(way))
            def _():
                z_copy(z, way, n).start()

        x_copy(z, x, n).start()
        if n == 0:
            for i in range(6):
                b_copy(c, i).start()
    for k in range(1, ep_count):
        s_copy(k).start()

    def forward(zb, n):
        way = jnp.where(zb < z, 0, 1)
        z_copy(zb, way, n).wait_recv()

        @pl.when(can_go(way))
        def _():
            z_copy(zb, way, n).start()

        x_copy(zb, x, n).start()

    def keys(zb):
        kz_copy(zb).wait_recv()

        @pl.when(z + 1 < lines)
        def _():
            kz_copy(zb).start()

        kx_copy(zb, x).start()

    def own_keys():
        load(3).wait()
        load(4).wait()

        @pl.when(z + 1 < lines)
        def _():
            kz_copy(z).start()

        @pl.when(x == 0)
        def _():
            kx_copy(z, x).start()

    def pass_on(zb, n):
        x_copy(zb, 1 - x, n).wait_recv()
        e_copy(zb, n).start()

    def gated_product(rows_in, gate_weight, up_weight):
        gate = jnp.dot(rows_in, gate_weight, preferred_element_type=wide)
        up = jnp.dot(rows_in, up_weight, preferred_element_type=wide)
        return (gate / (1.0 + jnp.exp(-gate)) * up).astype(low)

    def activate(zb, far, first):
        @pl.when(first == 1)
        def _():
            for n in (1, 2):
                load(n).wait()
                b_copy(1 - c, n - 1).wait_recv()

        @pl.when(far == 1)
        def _():
            for n in range(chunks):
                e_copy(zb, n).wait_recv()

        block = zb * 2 + jnp.where(far == 1, 1 - x, x)
        for h in range(2):
            act[block, y, :, h * units : (h + 1) * units] = gated_product(
                tok[block], gall[h], uall[h]
            )
        a_copy(block, y).start()

    def finish(zb, far, n):
        block = zb * 2 + jnp.where(far == 1, 1 - x, x)

        @pl.when(n == 0)
        def _():
            a_copy(block, 1 - y).wait_recv()

        weight = jnp.sum(
            jnp.where(at_row == at_lane, side[block, pl.ds(me, 1), :], 0.0), axis=1, keepdims=True
        )
        cols = lanes(n * piece, piece)
        total = jnp.dot(act[block, 0], dall[0, :, cols], preferred_element_type=wide)
        total += jnp.dot(act[block, 1], dall[1, :, cols], preferred_element_type=wide)
        res[block, :, cols] = (total * weight).astype(low)

        @pl.when(far == 1)
        def _():
            xo_copy(zb, n).start()

    def send_home(zb, n):
        cols = lanes(n * piece, piece)
        xo_copy(zb, n).wait_recv()
        zout[zb, :, cols] = (
            res[zb * 2 + x, :, cols].astype(wide) + xin[zb, :, cols].astype(wide)
        ).astype(low)
        zo_copy(zb, n).start()

    def memory(zb):
        @pl.when(zb * 2 + 1 - x < me)
        def _():
            kx_copy(zb, 1 - x).wait_recv()

        def one(n, carry):
            block = zb * 2 + n

            @pl.when(block <= me)
            def _():
                scores = lax.dot_general(
                    qb[...], kvb[block, :, :key_dim], (((1,), (1,)), ((), ())),
                    preferred_element_type=wide,
                ) * (key_dim ** -0.5)
                seen = (block < me) | (at_row >= at_lane)
                shown = jnp.where(seen, brow[block, 0:1, :] - stab[...], lowest)
                weights = jnp.where(seen, scores * jnp.exp(shown), 0.0)
                num[...] += jnp.dot(
                    weights.astype(low), kvb[block, :, key_dim:], preferred_element_type=wide
                )
                den[...] += jnp.broadcast_to(
                    jnp.sum(weights, axis=1, keepdims=True), den.shape
                )

            return carry

        lax.fori_loop(0, 2, one, 0)

    def shared_hidden():
        for n in (2, 3):
            load(n + 6).wait()
            b_copy(1 - c, n).wait_recv()
        for h in range(2):
            sall[y, :, h * shared : (h + 1) * shared] = gated_product(
                tok[me], sgall[h], suall[h]
            )
        y_copy(y, 2).start()

    def team():
        y_copy(1 - y, 0).wait_recv()
        f_copy(c, 0).start()
        for k in range(1, ep_count):
            s_arrival(k).wait_recv()
        gap = jnp.zeros((1, length), wide)
        top = jnp.full((1, length), lowest, wide)
        for b in reversed(range(ep_count)):
            earlier = b < me
            gap = jnp.where(earlier, gap + side[b, ep_count + 1 : ep_count + 2, :], gap)
            row = side[b, ep_count : ep_count + 1, :] + gap
            brow[b, 0:1, :] = row
            top = jnp.where(earlier, jnp.maximum(top, row), top)
        own = side[me, ep_count : ep_count + 1, :]
        within = jnp.max(jnp.where(at_row >= at_lane, own, lowest), axis=1, keepdims=True)
        before = jnp.max(jnp.maximum(top, gap), axis=1, keepdims=True)
        stab[...] = jnp.broadcast_to(jnp.maximum(within, before), stab.shape)
        num[...] = jnp.zeros_like(num)
        den[...] = jnp.zeros_like(den)
        load(6).wait()
        load(5).wait()
        b_copy(1 - c, 4).wait_recv()

    def project():
        load(7).wait()
        load(11).wait()
        hidden = num[...] / jnp.maximum(jnp.abs(den[:, 0:1]), den_floor)
        gated = (hidden * (1.0 / (1.0 + jnp.exp(-ogb[...].astype(wide))))).astype(low)
        for n in range(4):
            cols = slice(n * half // 2, (n + 1) * half // 2)
            mpart[:, cols] = jnp.dot(gated, mwb[:, cols], preferred_element_type=wide).astype(low)
        m_copy(c, 0).start()

    def pair():
        m_copy(c, 0).wait_recv()
        msum[...] = (
            mpart[sublanes(c * part, part), :].astype(wide) + mpeer[...].astype(wide)
        ).astype(low)
        m_copy(c, 1).start()

    def projected():
        m_copy(c, 1).wait_recv()
        mo_ref[sublanes(c * part, part), :] = (
            msum[...].astype(wide) + mother[...].astype(wide)
        ).astype(low)
        m_copy(c, 2).start()

    def shared_team():
        y_copy(1 - y, 1).wait_recv()
        f_copy(c, 1).start()
        y_copy(1 - y, 2).wait_recv()
        load(10).wait()
        b_copy(1 - c, 5).wait_recv()

    def last(n):
        @pl.when(n == 0)
        def _():
            f_copy(1 - c, 1).wait_recv()

        cols = lanes(n * piece, piece)
        xo_copy(z, n).wait_recv()
        total = res[me, :, cols].astype(wide) + xin[z, :, cols].astype(wide)
        for k in range(2):
            total += jnp.dot(sall[k], sdall[k, :, cols], preferred_element_type=wide)
        for k in range(1, lines):
            source = lax.rem(z + k, lines)
            zo_arrival(source, n).wait_recv()
            total += zin[source, :, cols].astype(wide)
        eo_ref[sublanes(c * rows, rows), lanes(y * half + n * piece, piece)] = total.astype(low)
        ey_copy(y, n).start()
        eb_copy(c, n).start()

    events = {
        FORWARD: lambda zb, far, n: forward(zb, n),
        KEYS: lambda zb, far, n: keys(zb),
        PASS: lambda zb, far, n: pass_on(zb, n),
        ACTIVATE: activate,
        FINISH: finish,
        HOME: lambda zb, far, n: send_home(zb, n),
        MEMORY: lambda zb, far, n: memory(zb),
        DOWN: lambda zb, far, n: y_copy(y, 0).start(),
        OWN_KEYS: lambda zb, far, n: own_keys(),
        SHARED: lambda zb, far, n: shared_hidden(),
        SHARED_DOWN: lambda zb, far, n: y_copy(y, 1).start(),
        TEAM: lambda zb, far, n: team(),
        TEAM_DONE: lambda zb, far, n: f_copy(1 - c, 0).wait_recv(),
        PROJECT: lambda zb, far, n: project(),
        PAIR: lambda zb, far, n: pair(),
        PROJECTED: lambda zb, far, n: projected(),
        SHARED_TEAM: lambda zb, far, n: shared_team(),
        LAST: lambda zb, far, n: last(n),
    }
    longest = max(len(order) for order in plan)
    words = []
    for at in range(0, longest, 3):
        word = jnp.int32(0)
        for k, order in enumerate(plan):
            packed = 0
            for code in reversed((order + (1023,) * longest)[at : at + 3]):
                packed = packed * 1024 + code
            word = jnp.where(z == k, packed, word)
        words.append(word)

    def event(i, carry):
        at, place = lax.div(i, 3), lax.rem(i, 3)
        word = words[0]
        for k in range(1, len(words)):
            word = jnp.where(at == k, words[k], word)
        code = jnp.where(place == 0, word, jnp.where(place == 1, word // 1024, word // 1048576))
        code = lax.rem(code, 1024)
        kind, arg = lax.div(code, 8 * lines), lax.rem(code, 8 * lines)
        zb, far, n = lax.div(arg, 8), lax.rem(lax.div(arg, 4), 2), lax.rem(arg, 4)
        for k, work in events.items():

            @pl.when(kind == k)
            def _():
                work(zb, far, n)

        return carry

    lax.fori_loop(0, longest, event, 0)

    for n in range(halves):
        ey_copy(1 - y, n).wait_recv()
        ef_copy(c, n).start()
    m_copy(1 - c, 2).wait_recv()
    for n in range(halves):
        eb_copy(1 - c, n).wait_recv()
        ef_copy(1 - c, n).wait_recv()

    for n in range(6):
        b_copy(c, n).wait_send()
    for n in range(3):
        y_copy(y, n).wait_send()
        m_copy(c, n).wait_send()
    for n in range(2):
        f_copy(c, n).wait_send()
    for n in range(halves):
        ey_copy(y, n).wait_send()
        eb_copy(c, n).wait_send()
        ef_copy(c, n).wait_send()
    for k in range(1, ep_count):
        s_copy(k).wait_send()

    @pl.when(x == 0)
    def _():
        kx_copy(z, x).wait_send()

    def drain(zb, carry):
        for way in range(2):
            passing = (zb <= z) if way == 0 else (zb >= z)

            @pl.when(can_go(way) & passing)
            def _():
                for n in range(chunks):
                    z_copy(zb, way, n).wait_send()

        @pl.when((z + 1 < lines) & (zb <= z))
        def _():
            kz_copy(zb).wait_send()

        @pl.when(zb < z)
        def _():
            kx_copy(zb, x).wait_send()

        for n in range(chunks):
            x_copy(zb, x, n).wait_send()
            e_copy(zb, n).wait_send()
        for n in range(halves):
            xo_copy(zb, n).wait_send()

            @pl.when(zb != z)
            def _():
                zo_copy(zb, n).wait_send()

        for n in range(2):
            a_copy(zb * 2 + n, y).wait_send()
        return carry

    lax.fori_loop(0, lines, drain, 0)


def lane_program(
    queries, key_vectors, values, out_gate, input_gate, forget_gate, mix_weight,
    expert_input, norm_gain, route_ids, route_weights, expert_gate, expert_up, expert_down,
    shared_gate, shared_up, shared_down,
):
    ep_count = lax.axis_size("ep")
    lines = ep_count // 2
    tokens, width = expert_input.shape
    rows, half = tokens // 2, width // 2
    length, channels = values.shape
    units, shared = expert_gate.shape[2], shared_gate.shape[1]
    low, wide, dma = jnp.bfloat16, jnp.float32, pltpu.SemaphoreType.DMA
    side_rows = ep_count + 2 + -(ep_count + 2) % 8
    vmem = pl.BlockSpec(memory_space=pltpu.VMEM)
    hbm = pl.BlockSpec(memory_space=pl.ANY)

    def buffer(*shape, dtype=low):
        return pltpu.VMEM(shape, dtype)

    return pl.pallas_call(
        functools.partial(lane_kernel, lines, PLANS[lines]),
        out_shape=(
            jax.ShapeDtypeStruct((length, width), low),
            jax.ShapeDtypeStruct((tokens, width), low),
        ),
        in_specs=[vmem] * 5 + [hbm] * 12,
        out_specs=(vmem, vmem),
        scratch_shapes=[
            buffer(rows, width),
            buffer(length, KEY_DIM),
            buffer(length, channels),
            buffer(channels, width),
            buffer(2, width, units),
            buffer(2, width, units),
            buffer(2, 2 * units, half),
            buffer(2, width, shared),
            buffer(2, width, shared),
            buffer(2, 2 * shared, half),
            buffer(2, rows, 2 * shared),
            buffer(ep_count, rows, width),
            buffer(ep_count, 2, rows, 2 * units),
            buffer(ep_count, length, KEY_DIM + channels),
            buffer(ep_count, side_rows, rows, dtype=wide),
            buffer(ep_count, 8, length, dtype=wide),
            buffer(length, length, dtype=wide),
            buffer(length, channels, dtype=wide),
            buffer(length, 128, dtype=wide),
            buffer(ep_count, rows, half),
            buffer(lines, rows, half),
            buffer(lines, rows, half),
            buffer(lines, rows, half),
            buffer(length, width),
            buffer(length // 2, width),
            buffer(length // 2, width),
            buffer(length // 2, width),
            dma((12,)),
            dma((2, lines, chunks)), dma((lines, chunks)),
            dma((lines, chunks)), dma((lines, chunks)),
            dma((lines, chunks)), dma((lines, chunks)),
            dma((lines,)), dma((lines,)), dma((lines,)), dma((lines,)),
            dma((ep_count - 1,)), dma((ep_count,)),
            dma((ep_count,)), dma((ep_count,)),
            dma((6,)), dma((6,)), dma((3,)), dma((3,)), dma((2,)), dma((2,)),
            dma((lines, halves)), dma((lines, halves)),
            dma((lines, halves)), dma((lines, halves)),
            dma((halves,)), dma((halves,)), dma((halves,)), dma((halves,)),
            dma((halves,)), dma((halves,)),
            dma((3,)), dma((3,)),
        ],
        compiler_params=pltpu.CompilerParams(
            collective_id=0, has_side_effects=True, vmem_limit_bytes=56 * 1024 * 1024
        ),
    )(
        input_gate.T, forget_gate.T, norm_gain[None, :], route_ids.T, route_weights.T,
        queries, key_vectors, values, out_gate, mix_weight, expert_input,
        expert_gate, expert_up, expert_down, shared_gate, shared_up, shared_down,
    )


def expert_half(
    expert_input,
    norm_gain,
    route_ids,
    route_weights,
    expert_gate,
    expert_up,
    expert_down,
    shared_gate,
    shared_up,
    shared_down,
):
    ep_count = lax.axis_size("ep")
    tp_count = lax.axis_size("tp")
    tp_rank = lax.axis_index("tp")
    tokens = expert_input.shape[0]
    top_count = route_ids.shape[1]
    slice_units = expert_gate.shape[2]
    group_size = FF // slice_units
    per_ep = tp_count // group_size
    team_index = tp_rank // group_size
    expert_count = ep_count * per_ep
    capacity = 2 * tokens * top_count // expert_count
    rows_wide = expert_input.astype(jnp.float32)
    normed = (
        rows_wide
        * lax.rsqrt(jnp.mean(rows_wide * rows_wide, axis=-1, keepdims=True) + epsilon)
        * norm_gain
    ).astype(jnp.bfloat16)
    chosen = route_ids.reshape(-1)
    onehot = (chosen[:, None] == jnp.arange(expert_count, dtype=jnp.int32)[None, :]).astype(
        jnp.int32
    )
    slot_rank = jnp.sum((jnp.cumsum(onehot, axis=0) - onehot) * onehot, axis=1)
    in_team = chosen % per_ep == team_index
    target = jnp.where(in_team, chosen // per_ep * capacity + slot_rank, ep_count * capacity)
    token_of = jnp.arange(chosen.shape[0], dtype=jnp.int32) // top_count
    slot_token = jnp.zeros((ep_count * capacity,), jnp.int32).at[target].set(token_of, mode="drop")
    slot_live = jnp.zeros((ep_count * capacity,), jnp.int32).at[target].set(1, mode="drop")
    outgoing = jnp.where(slot_live[:, None] > 0, normed[slot_token], jnp.zeros((), jnp.bfloat16))
    outgoing = outgoing.reshape(ep_count, capacity, D)
    gate_slice = expert_gate[0]
    up_slice = expert_up[0]
    down_slice = expert_down[0]
    arrived = lax.all_to_all(outgoing, "ep", split_axis=0, concat_axis=0, tiled=True)
    gate_val = jnp.einsum("sid,df->sif", arrived, gate_slice, preferred_element_type=jnp.float32)
    up_val = jnp.einsum("sid,df->sif", arrived, up_slice, preferred_element_type=jnp.float32)
    hidden = (jax.nn.silu(gate_val) * up_val).astype(jnp.bfloat16)
    partial_value = jnp.einsum(
        "sif,fd->sid", hidden, down_slice, preferred_element_type=jnp.float32
    )
    partial_value = partial_value.astype(jnp.bfloat16)
    returned = lax.all_to_all(partial_value, "ep", split_axis=0, concat_axis=0, tiled=True)
    flat_back = returned.reshape(ep_count * capacity, returned.shape[2])
    gather_at = jnp.where(in_team, target, 0).reshape(tokens, top_count)
    weight_at = jnp.where(in_team, route_weights.reshape(-1), 0.0).reshape(tokens, top_count)
    combined = jnp.zeros((tokens, returned.shape[2]), jnp.float32)
    for pick_index in range(top_count):
        combined = (
            combined
            + flat_back[gather_at[:, pick_index]].astype(jnp.float32)
            * weight_at[:, pick_index][:, None]
        )
    shared_gate_val = jnp.dot(normed, shared_gate, preferred_element_type=jnp.float32)
    shared_up_val = jnp.dot(normed, shared_up, preferred_element_type=jnp.float32)
    shared_act = (jax.nn.silu(shared_gate_val) * shared_up_val).astype(jnp.bfloat16)
    return combined + jnp.dot(shared_act, shared_down, preferred_element_type=jnp.float32)


def shards(
    queries,
    key_vectors,
    values,
    out_gate,
    input_gate,
    forget_gate,
    mix_weight,
    expert_input,
    norm_gain,
    route_ids,
    route_weights,
    expert_gate,
    expert_up,
    expert_down,
    shared_gate,
    shared_up,
    shared_down,
):
    ep_count, tp_count = lax.axis_size("ep"), lax.axis_size("tp")
    tokens, slots = expert_input.shape[0], route_ids.shape[1] * 2 * expert_input.shape[0]
    per_ep = tp_count * expert_gate.shape[2] // FF
    even = ep_count % 2 == 0 and tp_count == 4 and MEMORY_HEADS * 2 == tp_count
    blocked = values.shape[0] == BLOCK and tokens == 2 * BLOCK and ep_count // 2 in PLANS
    dense = even and blocked and per_ep == 1 and slots // (ep_count * per_ep) >= tokens
    experts = (
        expert_input,
        norm_gain,
        route_ids,
        route_weights,
        expert_gate,
        expert_up,
        expert_down,
        shared_gate,
        shared_up,
        shared_down,
    )
    if dense:
        return lane_program(
            queries, key_vectors, values, out_gate, input_gate, forget_gate, mix_weight, *experts
        )
    query_head, both, gates = mixer_local(
        queries, key_vectors, values, input_gate, forget_gate
    )
    both = lax.all_gather(both, "ep", axis=0, tiled=True)
    gates = lax.all_gather(gates, "ep", axis=1, tiled=True)
    gated_rows = mixer_rows(query_head, both, gates, out_gate)
    mixer_partial = jnp.dot(gated_rows, mix_weight, preferred_element_type=jnp.float32)
    expert_partial = expert_half(*experts)
    mixer_piece = lax.psum_scatter(
        mixer_partial.astype(jnp.bfloat16), "tp", scatter_dimension=0, tiled=True
    )
    mixer_out = lax.all_gather(mixer_piece, "tp", axis=0, tiled=True)
    expert_piece = lax.psum_scatter(expert_partial, "tp", scatter_dimension=0, tiled=True).astype(
        jnp.bfloat16
    )
    expert_out = lax.all_gather(expert_piece, "tp", axis=0, tiled=True)
    return (mixer_out, expert_out)


def solution(mesh):
    return jax.shard_map(
        shards,
        mesh=mesh,
        in_specs=(
            P("ep", None),
            P("ep", None),
            P("ep", "tp"),
            P("ep", "tp"),
            P("ep", None),
            P("ep", None),
            P("tp", None),
            P("ep", None),
            P(),
            P("ep", None),
            P("ep", None),
            P(("ep", "tp"), None, None),
            P(("ep", "tp"), None, None),
            P(("ep", "tp"), None, None),
            P(None, "tp"),
            P(None, "tp"),
            P("tp", None),
        ),
        out_specs=(P("ep", None), P("ep", None)),
        check_vma=False,
    )
```

```python
import functools

import jax
import jax.numpy as jnp
from jax import lax
from jax.experimental import pallas as pl
from jax.experimental.pallas import tpu as pltpu
from jax.sharding import PartitionSpec as P

D = 2048
MEMORY_HEADS = 2
KEY_DIM = 256
BLOCK = 128
FF = 1024


epsilon = 1e-06
lowest = -1e30
den_floor = 4.0


def mixer_local(queries, key_vectors, values, input_gate, forget_gate):
    tp_count = lax.axis_size("tp")
    tp_rank = lax.axis_index("tp")
    head_index = tp_rank // (tp_count // MEMORY_HEADS)
    offset = head_index * KEY_DIM
    query_head = lax.dynamic_slice_in_dim(queries, offset, KEY_DIM, 1)
    key_head = lax.dynamic_slice_in_dim(key_vectors, offset, KEY_DIM, 1)
    select = jnp.arange(MEMORY_HEADS, dtype=jnp.int32)[None, :] == head_index
    gates = jnp.stack(
        [
            jnp.sum(jnp.where(select, input_gate, 0.0), axis=1),
            jax.nn.log_sigmoid(jnp.sum(jnp.where(select, forget_gate, 0.0), axis=1)),
        ]
    )
    return query_head, jnp.concatenate([key_head, values], axis=1), gates


def mixer_rows(query_head, both, gates, out_gate):
    ep_count = lax.axis_size("ep")
    ep_rank = lax.axis_index("ep")
    length = query_head.shape[0]
    factor = KEY_DIM ** (-0.5)
    keys_all = both[:, :KEY_DIM]
    values_all = both[:, KEY_DIM:]
    total = ep_count * length
    blocks = total // BLOCK
    mine = length // BLOCK
    input_all = gates[0].reshape(blocks, BLOCK)
    cumulative = jnp.cumsum(gates[1].reshape(blocks, BLOCK), axis=1)
    block_total = cumulative[:, -1]
    index = jnp.arange(blocks, dtype=jnp.int32)
    here = ep_rank * mine + jnp.arange(mine, dtype=jnp.int32)
    between = (index[None, None, :] > index[None, :, None]) & (
        index[None, None, :] < here[:, None, None]
    )
    gap = jnp.sum(jnp.where(between, block_total[None, None, :], 0.0), axis=2)
    ahead = jnp.sum(jnp.where(index[None, :] < here[:, None], block_total[None, :], 0.0), axis=1)
    keep = block_total[:, None] - cumulative + input_all
    own_cumulative = lax.dynamic_slice_in_dim(cumulative, ep_rank * mine, mine, 0)
    same = index[None, :] == here[:, None]
    column = jnp.where(same[:, :, None], input_all - cumulative, keep + gap[:, :, None])
    log_weight = own_cumulative[:, :, None, None] + column[:, None]
    row_at = jnp.arange(BLOCK, dtype=jnp.int32)
    visible = (index[None, :] < here[:, None])[:, None, :, None] | (
        same[:, None, :, None] & (row_at[None, :, None, None] >= row_at[None, None, None, :])
    )
    log_weight = jnp.where(visible, log_weight, -jnp.inf).reshape(length, total)
    carried = (own_cumulative + ahead[:, None]).reshape(length)
    stabilizer = jnp.maximum(carried, jnp.max(log_weight, axis=1))
    within = jnp.exp(log_weight - stabilizer[:, None])
    scores = (
        jnp.einsum("td,sd->ts", query_head, keys_all, preferred_element_type=jnp.float32) * factor
    )
    weights = scores * within
    numerator = jnp.dot(
        weights.astype(jnp.bfloat16), values_all, preferred_element_type=jnp.float32
    )
    denominator = jnp.sum(weights, axis=1)
    hidden = numerator / jnp.maximum(jnp.abs(denominator), den_floor)[:, None]
    gated_rows = (hidden * jax.nn.sigmoid(out_gate.astype(jnp.float32))).astype(jnp.bfloat16)
    return gated_rows


chunks = 2
alone = 16
halves = 2
kinds = 18
(
    FORWARD, KEYS, PASS, ACTIVATE, FINISH, HOME, MEMORY, DOWN, OWN_KEYS,
    SHARED, SHARED_DOWN, TEAM, TEAM_DONE, PROJECT, PAIR, PROJECTED, SHARED_TEAM, LAST,
) = range(kinds)
PLANS = {
    4: (
        (
            224, 256, 97, 8, 288, 65, 9, 352, 104, 72, 16, 384, 73, 136, 128, 17,
            129, 64, 108, 80, 24, 81, 116, 25, 112, 192, 88, 416, 120, 148, 149, 89,
            140, 141, 137, 100, 144, 145, 176, 177, 124, 152, 168, 448, 169, 156, 153, 157,
            320, 184, 132, 133, 185, 512, 544, 545, 480,
        ),
        (
            224, 16, 0, 288, 105, 17, 112, 80, 1, 352, 384, 96, 136, 24, 73, 81,
            25, 128, 137, 256, 144, 64, 32, 65, 145, 116, 88, 100, 89, 72, 148, 149,
            120, 132, 133, 124, 108, 176, 192, 320, 200, 416, 156, 157, 152, 160, 140, 129,
            448, 184, 161, 512, 141, 177, 153, 185, 544, 545, 480,
        ),
        (
            224, 24, 80, 8, 113, 9, 25, 81, 120, 352, 384, 104, 0, 72, 73, 88,
            1, 96, 89, 136, 108, 40, 124, 152, 153, 32, 64, 288, 140, 65, 137, 116,
            256, 141, 156, 157, 100, 128, 129, 168, 320, 208, 200, 169, 192, 132, 133, 184,
            416, 448, 185, 148, 160, 512, 149, 161, 144, 145, 544, 480, 545,
        ),
        (
            224, 121, 16, 288, 17, 112, 256, 88, 80, 8, 81, 9, 352, 72, 116, 0,
            73, 104, 384, 144, 148, 108, 1, 96, 145, 136, 40, 89, 152, 176, 140, 141,
            32, 64, 65, 153, 124, 128, 100, 48, 149, 168, 200, 137, 320, 169, 216, 192,
            132, 133, 208, 416, 177, 448, 160, 156, 157, 129, 161, 512, 544, 545, 480,
        ),
    ),
}


def lane_kernel(
    lines, plan,
    ig_ref, fg_ref, gain_ref, ids_ref, rw_ref,
    q_ref, k_ref, v_ref, og_ref, mw_ref, x_ref, g_ref, u_ref, d_ref, sg_ref, su_ref, sd_ref,
    mo_ref, eo_ref,
    xbuf, qb, ogb, mwb, gall, uall, dall, sgall, suall, sdall, sall,
    tok, act, kvb, side, brow, stab, num, den, res, xin, zout, zin, mpart, mpeer, msum, mother,
    local, z_send, z_recv, x_send, x_recv, e_send, e_recv, kz_send, kz_recv, kx_send, kx_recv,
    s_send, s_recv, a_send, a_recv, b_send, b_recv, y_send, y_recv, f_send, f_recv,
    xo_send, xo_recv, zo_send, zo_recv, ey_send, ey_recv, eb_send, eb_recv, ef_send, ef_recv,
    m_send, m_recv,
):
    me = lax.axis_index("ep")
    j = lax.axis_index("tp")
    z, x = me // 2, me % 2
    y, c = j // 2, j % 2
    ep_count = 2 * lines
    rows = x_ref.shape[0] // 2
    length = q_ref.shape[0]
    key_dim = qb.shape[1]
    half = dall.shape[2]
    units = g_ref.shape[2]
    shared = sg_ref.shape[1]
    piece = half // halves
    part = length // 2
    low, wide = jnp.bfloat16, jnp.float32

    def remote(src, dst, send, recv, ep, tp):
        return pltpu.make_async_remote_copy(
            src_ref=src, dst_ref=dst, send_sem=send, recv_sem=recv,
            device_id={"ep": ep, "tp": tp}, device_id_type=pl.DeviceIdType.MESH,
        )

    across = z * 2 + 1 - x
    other_y = (1 - y) * 2 + c
    buddy = y * 2 + 1 - c

    def lanes(start, size):
        return pl.ds(pl.multiple_of(start, 128), size)

    def sublanes(start, size):
        return pl.ds(pl.multiple_of(start, 8), size)

    mine = lanes(y * half, half)
    theirs = lanes((1 - y) * half, half)
    heads = lanes(y * key_dim, key_dim)

    def load(n):
        pairs = (
            (x_ref.at[sublanes(c * rows, rows)], xbuf),
            (g_ref.at[0], gall.at[c]),
            (u_ref.at[0], uall.at[c]),
            (k_ref.at[:, heads], kvb.at[me, :, :key_dim]),
            (v_ref, kvb.at[me, :, key_dim:]),
            (d_ref.at[0, :, mine], dall.at[y, sublanes(c * units, units)]),
            (q_ref.at[:, heads], qb),
            (og_ref, ogb),
            (sg_ref, sgall.at[c]),
            (su_ref, suall.at[c]),
            (sd_ref.at[:, mine], sdall.at[y, sublanes(c * shared, shared)]),
            (mw_ref, mwb),
        )
        return pltpu.make_async_copy(*pairs[n], local.at[n])

    for n in range(12):
        load(n).start()

    barrier = pltpu.get_barrier_semaphore()

    def greet(ep, tp):
        pl.semaphore_signal(
            barrier, inc=1, device_id={"ep": ep, "tp": tp}, device_id_type=pl.DeviceIdType.MESH
        )

    for k in range(1, ep_count):
        greet(lax.rem(me + k, ep_count), j)
    greet(me, other_y)
    greet(me, buddy)

    chunk = rows // chunks

    def z_copy(zb, way, n):
        ref = tok.at[zb * 2 + x, sublanes(n * chunk, chunk)]
        to = z + 1 - 2 * way
        return remote(ref, ref, z_send.at[way, zb, n], z_recv.at[zb, n], to * 2 + x, j)

    def x_copy(zb, column, n):
        ref = tok.at[zb * 2 + column, sublanes(n * chunk + y * alone, chunk - alone)]
        return remote(ref, ref, x_send.at[zb, n], x_recv.at[zb, n], across, j)

    def e_copy(zb, n):
        ref = tok.at[zb * 2 + 1 - x, sublanes(n * chunk + y * (chunk - alone), alone)]
        return remote(ref, ref, e_send.at[zb, n], e_recv.at[zb, n], me, other_y)

    def kz_copy(zb):
        ref = kvb.at[zb * 2 + x]
        return remote(ref, ref, kz_send.at[zb], kz_recv.at[zb], (z + 1) * 2 + x, j)

    def kx_copy(zb, column):
        ref = kvb.at[zb * 2 + column]
        return remote(ref, ref, kx_send.at[zb], kx_recv.at[zb], across, j)

    def s_copy(k):
        return remote(
            side.at[me], side.at[me], s_send.at[k - 1], s_recv.at[me], lax.rem(me + k, ep_count), j
        )

    def s_arrival(k):
        source = lax.rem(me + k, ep_count)
        return remote(
            side.at[source], side.at[source], s_send.at[k - 1], s_recv.at[source], source, j
        )

    def a_copy(block, team):
        ref = act.at[block, team]
        return remote(ref, ref, a_send.at[block], a_recv.at[block], me, other_y)

    def b_copy(core, n):
        pairs = (
            (g_ref.at[0], gall.at[core]),
            (u_ref.at[0], uall.at[core]),
            (sg_ref, sgall.at[core]),
            (su_ref, suall.at[core]),
            (d_ref.at[0, :, mine], dall.at[y, sublanes(core * units, units)]),
            (sd_ref.at[:, mine], sdall.at[y, sublanes(core * shared, shared)]),
        )
        return remote(*pairs[n], b_send.at[n], b_recv.at[n], me, buddy)

    def y_copy(team, n):
        pairs = (
            (d_ref.at[0, :, theirs], dall.at[team, sublanes(c * units, units)]),
            (sd_ref.at[:, theirs], sdall.at[team, sublanes(c * shared, shared)]),
            (sall.at[team], sall.at[team]),
        )
        return remote(*pairs[n], y_send.at[n], y_recv.at[n], me, other_y)

    def f_copy(core, n):
        refs = (
            dall.at[1 - y, sublanes(core * units, units)],
            sdall.at[1 - y, sublanes(core * shared, shared)],
        )
        return remote(refs[n], refs[n], f_send.at[n], f_recv.at[n], me, buddy)

    def xo_copy(zb, n):
        cols = lanes(n * piece, piece)
        return remote(
            res.at[zb * 2 + 1 - x, :, cols], xin.at[zb, :, cols],
            xo_send.at[zb, n], xo_recv.at[zb, n], across, j,
        )

    def zo_copy(zb, n):
        cols = lanes(n * piece, piece)
        return remote(
            zout.at[zb, :, cols], zin.at[z, :, cols],
            zo_send.at[zb, n], zo_recv.at[z, n], zb * 2 + x, j,
        )

    def zo_arrival(zb, n):
        cols = lanes(n * piece, piece)
        return remote(
            zout.at[zb, :, cols], zin.at[zb, :, cols],
            zo_send.at[zb, n], zo_recv.at[zb, n], zb * 2 + x, j,
        )

    def final(core, team, n):
        return eo_ref.at[
            sublanes(core * rows, rows), lanes(team * half + n * piece, piece)
        ]

    def ey_copy(team, n):
        ref = final(c, team, n)
        return remote(ref, ref, ey_send.at[n], ey_recv.at[n], me, other_y)

    def eb_copy(core, n):
        ref = final(core, y, n)
        return remote(ref, ref, eb_send.at[n], eb_recv.at[n], me, buddy)

    def ef_copy(core, n):
        ref = final(core, 1 - y, n)
        return remote(ref, ref, ef_send.at[n], ef_recv.at[n], me, buddy)

    def m_copy(core, n):
        ref = mo_ref.at[sublanes(core * part, part)]
        pairs = (
            (mpart.at[sublanes((1 - c) * part, part)], mpeer, buddy),
            (msum, mother, other_y),
            (ref, ref, buddy),
        )
        source, target, to = pairs[n]
        return remote(source, target, m_send.at[n], m_recv.at[n], me, to)

    at_row = lax.broadcasted_iota(jnp.int32, (length, length), 0)
    at_lane = lax.broadcasted_iota(jnp.int32, (length, length), 1)
    token_lanes = lanes(c * rows, rows)
    ids = ids_ref[:, token_lanes]
    route = rw_ref[:, token_lanes]
    for e in range(ep_count):
        side[me, e : e + 1, :] = jnp.sum(jnp.where(ids == e, route, 0.0), axis=0, keepdims=True)
    forget = fg_ref[pl.ds(y, 1), :]
    small = jnp.exp(-jnp.abs(forget))
    kept = jnp.minimum(forget, 0.0) - jnp.log1p(small)
    kept_column = jnp.sum(jnp.where(at_row == at_lane, kept, 0.0), axis=1, keepdims=True)
    cumulative = jnp.sum(jnp.where(at_row <= at_lane, kept_column, 0.0), axis=0, keepdims=True)
    side[me, ep_count : ep_count + 1, :] = ig_ref[pl.ds(y, 1), :] - cumulative
    side[me, ep_count + 1 : ep_count + 2, :] = jnp.broadcast_to(
        jnp.sum(kept, axis=1, keepdims=True), (1, length)
    )

    def normalize(n):
        def group(i, carry):
            at_rows = sublanes(n * chunk + i * 16, 16)
            wide_rows = xbuf[at_rows, :].astype(wide)
            scale = lax.rsqrt(jnp.mean(wide_rows * wide_rows, axis=1, keepdims=True) + epsilon)
            tok[me, at_rows, :] = (wide_rows * scale * gain_ref[...]).astype(low)
            return carry

        lax.fori_loop(0, chunk // 16, group, 0)

    def can_go(way):
        to = z + 1 - 2 * way
        return (to >= 0) & (to < lines)

    load(0).wait()
    normalize(0)
    pl.semaphore_wait(barrier, ep_count + 1)
    for n in range(chunks):
        if n:
            normalize(n)
        for way in range(2):

            @pl.when(can_go(way))
            def _():
                z_copy(z, way, n).start()

        x_copy(z, x, n).start()
        if n == 0:
            for i in range(6):
                b_copy(c, i).start()
    for k in range(1, ep_count):
        s_copy(k).start()

    def forward(zb, n):
        way = jnp.where(zb < z, 0, 1)
        z_copy(zb, way, n).wait_recv()

        @pl.when(can_go(way))
        def _():
            z_copy(zb, way, n).start()

        x_copy(zb, x, n).start()

    def keys(zb):
        kz_copy(zb).wait_recv()

        @pl.when(z + 1 < lines)
        def _():
            kz_copy(zb).start()

        kx_copy(zb, x).start()

    def own_keys():
        load(3).wait()
        load(4).wait()

        @pl.when(z + 1 < lines)
        def _():
            kz_copy(z).start()

        @pl.when(x == 0)
        def _():
            kx_copy(z, x).start()

    def pass_on(zb, n):
        x_copy(zb, 1 - x, n).wait_recv()
        e_copy(zb, n).start()

    def gated_product(rows_in, gate_weight, up_weight):
        gate = jnp.dot(rows_in, gate_weight, preferred_element_type=wide)
        up = jnp.dot(rows_in, up_weight, preferred_element_type=wide)
        return (gate / (1.0 + jnp.exp(-gate)) * up).astype(low)

    def activate(zb, far, first):
        @pl.when(first == 1)
        def _():
            for n in (1, 2):
                load(n).wait()
                b_copy(1 - c, n - 1).wait_recv()

        @pl.when(far == 1)
        def _():
            for n in range(chunks):
                e_copy(zb, n).wait_recv()

        block = zb * 2 + jnp.where(far == 1, 1 - x, x)
        for h in range(2):
            act[block, y, :, h * units : (h + 1) * units] = gated_product(
                tok[block], gall[h], uall[h]
            )
        a_copy(block, y).start()

    def finish(zb, far, n):
        block = zb * 2 + jnp.where(far == 1, 1 - x, x)

        @pl.when(n == 0)
        def _():
            a_copy(block, 1 - y).wait_recv()

        weight = jnp.sum(
            jnp.where(at_row == at_lane, side[block, pl.ds(me, 1), :], 0.0), axis=1, keepdims=True
        )
        cols = lanes(n * piece, piece)
        total = jnp.dot(act[block, 0], dall[0, :, cols], preferred_element_type=wide)
        total += jnp.dot(act[block, 1], dall[1, :, cols], preferred_element_type=wide)
        res[block, :, cols] = (total * weight).astype(low)

        @pl.when(far == 1)
        def _():
            xo_copy(zb, n).start()

    def send_home(zb, n):
        cols = lanes(n * piece, piece)
        xo_copy(zb, n).wait_recv()
        zout[zb, :, cols] = (
            res[zb * 2 + x, :, cols].astype(wide) + xin[zb, :, cols].astype(wide)
        ).astype(low)
        zo_copy(zb, n).start()

    def memory(zb):
        @pl.when(zb * 2 + 1 - x < me)
        def _():
            kx_copy(zb, 1 - x).wait_recv()

        def one(n, carry):
            block = zb * 2 + n

            @pl.when(block <= me)
            def _():
                scores = lax.dot_general(
                    qb[...], kvb[block, :, :key_dim], (((1,), (1,)), ((), ())),
                    preferred_element_type=wide,
                ) * (key_dim ** -0.5)
                seen = (block < me) | (at_row >= at_lane)
                shown = jnp.where(seen, brow[block, 0:1, :] - stab[...], lowest)
                weights = jnp.where(seen, scores * jnp.exp(shown), 0.0)
                num[...] += jnp.dot(
                    weights.astype(low), kvb[block, :, key_dim:], preferred_element_type=wide
                )
                den[...] += jnp.broadcast_to(
                    jnp.sum(weights, axis=1, keepdims=True), den.shape
                )

            return carry

        lax.fori_loop(0, 2, one, 0)

    def shared_hidden():
        for n in (2, 3):
            load(n + 6).wait()
            b_copy(1 - c, n).wait_recv()
        for h in range(2):
            sall[y, :, h * shared : (h + 1) * shared] = gated_product(
                tok[me], sgall[h], suall[h]
            )
        y_copy(y, 2).start()

    def team():
        y_copy(1 - y, 0).wait_recv()
        f_copy(c, 0).start()
        for k in range(1, ep_count):
            s_arrival(k).wait_recv()
        gap = jnp.zeros((1, length), wide)
        top = jnp.full((1, length), lowest, wide)
        for b in reversed(range(ep_count)):
            earlier = b < me
            gap = jnp.where(earlier, gap + side[b, ep_count + 1 : ep_count + 2, :], gap)
            row = side[b, ep_count : ep_count + 1, :] + gap
            brow[b, 0:1, :] = row
            top = jnp.where(earlier, jnp.maximum(top, row), top)
        own = side[me, ep_count : ep_count + 1, :]
        within = jnp.max(jnp.where(at_row >= at_lane, own, lowest), axis=1, keepdims=True)
        before = jnp.max(jnp.maximum(top, gap), axis=1, keepdims=True)
        stab[...] = jnp.broadcast_to(jnp.maximum(within, before), stab.shape)
        num[...] = jnp.zeros_like(num)
        den[...] = jnp.zeros_like(den)
        load(6).wait()
        load(5).wait()
        b_copy(1 - c, 4).wait_recv()

    def project():
        load(7).wait()
        load(11).wait()
        hidden = num[...] / jnp.maximum(jnp.abs(den[:, 0:1]), den_floor)
        gated = (hidden * (1.0 / (1.0 + jnp.exp(-ogb[...].astype(wide))))).astype(low)
        for n in range(4):
            cols = slice(n * half // 2, (n + 1) * half // 2)
            mpart[:, cols] = jnp.dot(gated, mwb[:, cols], preferred_element_type=wide).astype(low)
        m_copy(c, 0).start()

    def pair():
        m_copy(c, 0).wait_recv()
        msum[...] = (
            mpart[sublanes(c * part, part), :].astype(wide) + mpeer[...].astype(wide)
        ).astype(low)
        m_copy(c, 1).start()

    def projected():
        m_copy(c, 1).wait_recv()
        mo_ref[sublanes(c * part, part), :] = (
            msum[...].astype(wide) + mother[...].astype(wide)
        ).astype(low)
        m_copy(c, 2).start()

    def shared_team():
        y_copy(1 - y, 1).wait_recv()
        f_copy(c, 1).start()
        y_copy(1 - y, 2).wait_recv()
        load(10).wait()
        b_copy(1 - c, 5).wait_recv()

    def last(n):
        @pl.when(n == 0)
        def _():
            f_copy(1 - c, 1).wait_recv()

        cols = lanes(n * piece, piece)
        xo_copy(z, n).wait_recv()
        total = res[me, :, cols].astype(wide) + xin[z, :, cols].astype(wide)
        for k in range(2):
            total += jnp.dot(sall[k], sdall[k, :, cols], preferred_element_type=wide)
        for k in range(1, lines):
            source = lax.rem(z + k, lines)
            zo_arrival(source, n).wait_recv()
            total += zin[source, :, cols].astype(wide)
        eo_ref[sublanes(c * rows, rows), lanes(y * half + n * piece, piece)] = total.astype(low)
        ey_copy(y, n).start()
        eb_copy(c, n).start()

    events = {
        FORWARD: lambda zb, far, n: forward(zb, n),
        KEYS: lambda zb, far, n: keys(zb),
        PASS: lambda zb, far, n: pass_on(zb, n),
        ACTIVATE: activate,
        FINISH: finish,
        HOME: lambda zb, far, n: send_home(zb, n),
        MEMORY: lambda zb, far, n: memory(zb),
        DOWN: lambda zb, far, n: y_copy(y, 0).start(),
        OWN_KEYS: lambda zb, far, n: own_keys(),
        SHARED: lambda zb, far, n: shared_hidden(),
        SHARED_DOWN: lambda zb, far, n: y_copy(y, 1).start(),
        TEAM: lambda zb, far, n: team(),
        TEAM_DONE: lambda zb, far, n: f_copy(1 - c, 0).wait_recv(),
        PROJECT: lambda zb, far, n: project(),
        PAIR: lambda zb, far, n: pair(),
        PROJECTED: lambda zb, far, n: projected(),
        SHARED_TEAM: lambda zb, far, n: shared_team(),
        LAST: lambda zb, far, n: last(n),
    }
    longest = max(len(order) for order in plan)
    words = []
    for at in range(0, longest, 3):
        word = jnp.int32(0)
        for k, order in enumerate(plan):
            packed = 0
            for code in reversed((order + (1023,) * longest)[at : at + 3]):
                packed = packed * 1024 + code
            word = jnp.where(z == k, packed, word)
        words.append(word)

    def event(i, carry):
        at, place = lax.div(i, 3), lax.rem(i, 3)
        word = words[0]
        for k in range(1, len(words)):
            word = jnp.where(at == k, words[k], word)
        code = jnp.where(place == 0, word, jnp.where(place == 1, word // 1024, word // 1048576))
        code = lax.rem(code, 1024)
        kind, arg = lax.div(code, 8 * lines), lax.rem(code, 8 * lines)
        zb, far, n = lax.div(arg, 8), lax.rem(lax.div(arg, 4), 2), lax.rem(arg, 4)

        def choose(low_kind, high_kind):
            if high_kind - low_kind == 1:
                events[low_kind](zb, far, n)
                return
            middle = (low_kind + high_kind) // 2

            @pl.when(kind < middle)
            def _():
                choose(low_kind, middle)

            @pl.when(kind >= middle)
            def _():
                choose(middle, high_kind)

        @pl.when(kind < kinds)
        def _():
            choose(0, kinds)

        return carry

    lax.fori_loop(0, longest, event, 0)

    for n in range(halves):
        ey_copy(1 - y, n).wait_recv()
        ef_copy(c, n).start()
    m_copy(1 - c, 2).wait_recv()
    for n in range(halves):
        eb_copy(1 - c, n).wait_recv()
        ef_copy(1 - c, n).wait_recv()

    for n in range(6):
        b_copy(c, n).wait_send()
    for n in range(3):
        y_copy(y, n).wait_send()
        m_copy(c, n).wait_send()
    for n in range(2):
        f_copy(c, n).wait_send()
    for n in range(halves):
        ey_copy(y, n).wait_send()
        eb_copy(c, n).wait_send()
        ef_copy(c, n).wait_send()
    for k in range(1, ep_count):
        s_copy(k).wait_send()

    @pl.when(x == 0)
    def _():
        kx_copy(z, x).wait_send()

    def drain(zb, carry):
        for way in range(2):
            passing = (zb <= z) if way == 0 else (zb >= z)

            @pl.when(can_go(way) & passing)
            def _():
                for n in range(chunks):
                    z_copy(zb, way, n).wait_send()

        @pl.when((z + 1 < lines) & (zb <= z))
        def _():
            kz_copy(zb).wait_send()

        @pl.when(zb < z)
        def _():
            kx_copy(zb, x).wait_send()

        for n in range(chunks):
            x_copy(zb, x, n).wait_send()
            e_copy(zb, n).wait_send()
        for n in range(halves):
            xo_copy(zb, n).wait_send()

            @pl.when(zb != z)
            def _():
                zo_copy(zb, n).wait_send()

        for n in range(2):
            a_copy(zb * 2 + n, y).wait_send()
        return carry

    lax.fori_loop(0, lines, drain, 0)


def write_kernel(mixed_ref, routed_ref, mo_ref, eo_ref, sem):
    copies = [
        pltpu.make_async_copy(routed_ref, eo_ref, sem.at[0]),
        pltpu.make_async_copy(mixed_ref, mo_ref, sem.at[1]),
    ]
    for copy in copies:
        copy.start()
    for copy in copies:
        copy.wait()


def lane_program(
    queries, key_vectors, values, out_gate, input_gate, forget_gate, mix_weight,
    expert_input, norm_gain, route_ids, route_weights, expert_gate, expert_up, expert_down,
    shared_gate, shared_up, shared_down,
):
    ep_count = lax.axis_size("ep")
    lines = ep_count // 2
    tokens, width = expert_input.shape
    rows, half = tokens // 2, width // 2
    length, channels = values.shape
    units, shared = expert_gate.shape[2], shared_gate.shape[1]
    low, wide, dma = jnp.bfloat16, jnp.float32, pltpu.SemaphoreType.DMA
    side_rows = ep_count + 2 + -(ep_count + 2) % 8
    vmem = pl.BlockSpec(memory_space=pltpu.VMEM)
    hbm = pl.BlockSpec(memory_space=pl.ANY)

    def buffer(*shape, dtype=low):
        return pltpu.VMEM(shape, dtype)

    results = pl.pallas_call(
        functools.partial(lane_kernel, lines, PLANS[lines]),
        out_shape=(
            jax.ShapeDtypeStruct((length, width), low),
            jax.ShapeDtypeStruct((tokens, width), low),
        ),
        in_specs=[vmem] * 5 + [pl.BlockSpec(memory_space=pltpu.HBM)] * 12,
        out_specs=(vmem, vmem),
        scratch_shapes=[
            buffer(rows, width),
            buffer(length, KEY_DIM),
            buffer(length, channels),
            buffer(channels, width),
            buffer(2, width, units),
            buffer(2, width, units),
            buffer(2, 2 * units, half),
            buffer(2, width, shared),
            buffer(2, width, shared),
            buffer(2, 2 * shared, half),
            buffer(2, rows, 2 * shared),
            buffer(ep_count, rows, width),
            buffer(ep_count, 2, rows, 2 * units),
            buffer(ep_count, length, KEY_DIM + channels),
            buffer(ep_count, side_rows, rows, dtype=wide),
            buffer(ep_count, 8, length, dtype=wide),
            buffer(length, length, dtype=wide),
            buffer(length, channels, dtype=wide),
            buffer(length, 128, dtype=wide),
            buffer(ep_count, rows, half),
            buffer(lines, rows, half),
            buffer(lines, rows, half),
            buffer(lines, rows, half),
            buffer(length, width),
            buffer(length // 2, width),
            buffer(length // 2, width),
            buffer(length // 2, width),
            dma((12,)),
            dma((2, lines, chunks)), dma((lines, chunks)),
            dma((lines, chunks)), dma((lines, chunks)),
            dma((lines, chunks)), dma((lines, chunks)),
            dma((lines,)), dma((lines,)), dma((lines,)), dma((lines,)),
            dma((ep_count - 1,)), dma((ep_count,)),
            dma((ep_count,)), dma((ep_count,)),
            dma((6,)), dma((6,)), dma((3,)), dma((3,)), dma((2,)), dma((2,)),
            dma((lines, halves)), dma((lines, halves)),
            dma((lines, halves)), dma((lines, halves)),
            dma((halves,)), dma((halves,)), dma((halves,)), dma((halves,)),
            dma((halves,)), dma((halves,)),
            dma((3,)), dma((3,)),
        ],
        compiler_params=pltpu.CompilerParams(
            collective_id=0, has_side_effects=True, vmem_limit_bytes=40 * 1024 * 1024
        ),
    )(
        *(
            pltpu.with_memory_space_constraint(array, pltpu.HBM)
            for array in (
                input_gate.T, forget_gate.T, norm_gain[None, :], route_ids.T, route_weights.T,
            )
        ),
        *(
            pltpu.with_memory_space_constraint(array, pltpu.HBM)
            for array in (
                queries, key_vectors, values, out_gate, mix_weight, expert_input,
                expert_gate, expert_up, expert_down, shared_gate, shared_up, shared_down,
            )
        ),
    )
    return pl.pallas_call(
        write_kernel,
        out_shape=(
            jax.ShapeDtypeStruct((length, width), low),
            jax.ShapeDtypeStruct((tokens, width), low),
        ),
        in_specs=[hbm, hbm],
        out_specs=(hbm, hbm),
        scratch_shapes=[dma((2,))],
        compiler_params=pltpu.CompilerParams(vmem_limit_bytes=1024 * 1024),
    )(*results)


def expert_half(
    expert_input,
    norm_gain,
    route_ids,
    route_weights,
    expert_gate,
    expert_up,
    expert_down,
    shared_gate,
    shared_up,
    shared_down,
):
    ep_count = lax.axis_size("ep")
    tp_count = lax.axis_size("tp")
    tp_rank = lax.axis_index("tp")
    tokens = expert_input.shape[0]
    top_count = route_ids.shape[1]
    slice_units = expert_gate.shape[2]
    group_size = FF // slice_units
    per_ep = tp_count // group_size
    team_index = tp_rank // group_size
    expert_count = ep_count * per_ep
    capacity = 2 * tokens * top_count // expert_count
    rows_wide = expert_input.astype(jnp.float32)
    normed = (
        rows_wide
        * lax.rsqrt(jnp.mean(rows_wide * rows_wide, axis=-1, keepdims=True) + epsilon)
        * norm_gain
    ).astype(jnp.bfloat16)
    chosen = route_ids.reshape(-1)
    onehot = (chosen[:, None] == jnp.arange(expert_count, dtype=jnp.int32)[None, :]).astype(
        jnp.int32
    )
    slot_rank = jnp.sum((jnp.cumsum(onehot, axis=0) - onehot) * onehot, axis=1)
    in_team = chosen % per_ep == team_index
    target = jnp.where(in_team, chosen // per_ep * capacity + slot_rank, ep_count * capacity)
    token_of = jnp.arange(chosen.shape[0], dtype=jnp.int32) // top_count
    slot_token = jnp.zeros((ep_count * capacity,), jnp.int32).at[target].set(token_of, mode="drop")
    slot_live = jnp.zeros((ep_count * capacity,), jnp.int32).at[target].set(1, mode="drop")
    outgoing = jnp.where(slot_live[:, None] > 0, normed[slot_token], jnp.zeros((), jnp.bfloat16))
    outgoing = outgoing.reshape(ep_count, capacity, D)
    gate_slice = expert_gate[0]
    up_slice = expert_up[0]
    down_slice = expert_down[0]
    arrived = lax.all_to_all(outgoing, "ep", split_axis=0, concat_axis=0, tiled=True)
    gate_val = jnp.einsum("sid,df->sif", arrived, gate_slice, preferred_element_type=jnp.float32)
    up_val = jnp.einsum("sid,df->sif", arrived, up_slice, preferred_element_type=jnp.float32)
    hidden = (jax.nn.silu(gate_val) * up_val).astype(jnp.bfloat16)
    partial_value = jnp.einsum(
        "sif,fd->sid", hidden, down_slice, preferred_element_type=jnp.float32
    )
    partial_value = partial_value.astype(jnp.bfloat16)
    returned = lax.all_to_all(partial_value, "ep", split_axis=0, concat_axis=0, tiled=True)
    flat_back = returned.reshape(ep_count * capacity, returned.shape[2])
    gather_at = jnp.where(in_team, target, 0).reshape(tokens, top_count)
    weight_at = jnp.where(in_team, route_weights.reshape(-1), 0.0).reshape(tokens, top_count)
    combined = jnp.zeros((tokens, returned.shape[2]), jnp.float32)
    for pick_index in range(top_count):
        combined = (
            combined
            + flat_back[gather_at[:, pick_index]].astype(jnp.float32)
            * weight_at[:, pick_index][:, None]
        )
    shared_gate_val = jnp.dot(normed, shared_gate, preferred_element_type=jnp.float32)
    shared_up_val = jnp.dot(normed, shared_up, preferred_element_type=jnp.float32)
    shared_act = (jax.nn.silu(shared_gate_val) * shared_up_val).astype(jnp.bfloat16)
    return combined + jnp.dot(shared_act, shared_down, preferred_element_type=jnp.float32)


def shards(
    queries,
    key_vectors,
    values,
    out_gate,
    input_gate,
    forget_gate,
    mix_weight,
    expert_input,
    norm_gain,
    route_ids,
    route_weights,
    expert_gate,
    expert_up,
    expert_down,
    shared_gate,
    shared_up,
    shared_down,
):
    ep_count, tp_count = lax.axis_size("ep"), lax.axis_size("tp")
    tokens, slots = expert_input.shape[0], route_ids.shape[1] * 2 * expert_input.shape[0]
    per_ep = tp_count * expert_gate.shape[2] // FF
    even = ep_count % 2 == 0 and tp_count == 4 and MEMORY_HEADS * 2 == tp_count
    blocked = values.shape[0] == BLOCK and tokens == 2 * BLOCK and ep_count // 2 in PLANS
    dense = even and blocked and per_ep == 1 and slots // (ep_count * per_ep) >= tokens
    experts = (
        expert_input,
        norm_gain,
        route_ids,
        route_weights,
        expert_gate,
        expert_up,
        expert_down,
        shared_gate,
        shared_up,
        shared_down,
    )
    if dense:
        return lane_program(
            queries, key_vectors, values, out_gate, input_gate, forget_gate, mix_weight, *experts
        )
    query_head, both, gates = mixer_local(
        queries, key_vectors, values, input_gate, forget_gate
    )
    both = lax.all_gather(both, "ep", axis=0, tiled=True)
    gates = lax.all_gather(gates, "ep", axis=1, tiled=True)
    gated_rows = mixer_rows(query_head, both, gates, out_gate)
    mixer_partial = jnp.dot(gated_rows, mix_weight, preferred_element_type=jnp.float32)
    expert_partial = expert_half(*experts)
    mixer_piece = lax.psum_scatter(
        mixer_partial.astype(jnp.bfloat16), "tp", scatter_dimension=0, tiled=True
    )
    mixer_out = lax.all_gather(mixer_piece, "tp", axis=0, tiled=True)
    expert_piece = lax.psum_scatter(expert_partial, "tp", scatter_dimension=0, tiled=True).astype(
        jnp.bfloat16
    )
    expert_out = lax.all_gather(expert_piece, "tp", axis=0, tiled=True)
    return (mixer_out, expert_out)


def solution(mesh):
    return jax.shard_map(
        shards,
        mesh=mesh,
        in_specs=(
            P("ep", None),
            P("ep", None),
            P("ep", "tp"),
            P("ep", "tp"),
            P("ep", None),
            P("ep", None),
            P("tp", None),
            P("ep", None),
            P(),
            P("ep", None),
            P("ep", None),
            P(("ep", "tp"), None, None),
            P(("ep", "tp"), None, None),
            P(("ep", "tp"), None, None),
            P(None, "tp"),
            P(None, "tp"),
            P("tp", None),
        ),
        out_specs=(P("ep", None), P("ep", None)),
        check_vma=False,
    )
```
